256 devices in a mesh: kv: 16 (over y, x), tp: 16 (over z, core).
Axes of the slice: x: 4, y: 4, z: 8, core: 2. Of those that a mesh axis runs over, the one named last changes fastest.
Arguments:
- tokens: bfloat16 [256, 4096], P(None, ('kv', 'tp')), may hold values from -6 to 6
- memory: float32 [256, 16, 256, 128], P('kv', 'tp'), may hold values from -6 to 6
- normalizer: float32 [256, 16, 128], P('kv', 'tp'), may hold values from -6 to 6
- stabilizer: float32 [256, 16], P('kv', 'tp'), may hold values from -4 to 4
- first_gain: float32 [4096], replicated, may hold values from 0.1 to 1.9
- first_gate: bfloat16 [4096, 12288], P('kv', 'tp'), may hold values from -0.09375 to 0.09375
- first_up: bfloat16 [4096, 12288], P('kv', 'tp'), may hold values from -0.09375 to 0.09375
- first_down: bfloat16 [12288, 4096], P('tp', 'kv'), may hold values from -0.078125 to 0.078125
- mixer_gain: float32 [4096], replicated, may hold values from 0.1 to 1.9
- query_weight: bfloat16 [4096, 2048], P(None, 'tp'), may hold values from -0.09375 to 0.09375
- key_weight: bfloat16 [4096, 2048], P(None, 'tp'), may hold values from -0.09375 to 0.09375
- value_weight: bfloat16 [4096, 4096], P(None, 'tp'), may hold values from -0.09375 to 0.09375
- input_weight: bfloat16 [4096, 16], replicated, may hold values from -0.09375 to 0.09375
- forget_weight: bfloat16 [4096, 16], replicated, may hold values from -0.09375 to 0.09375
- forget_bias: float32 [16], P('tp'), may hold values from -2 to 4
- output_weight: bfloat16 [4096, 4096], P('tp'), may hold values from -0.09375 to 0.09375
- last_gain: float32 [4096], replicated, may hold values from 0.1 to 1.9
- last_gate: bfloat16 [4096, 12288], P('kv', 'tp'), may hold values from -0.09375 to 0.09375
- last_up: bfloat16 [4096, 12288], P('kv', 'tp'), may hold values from -0.09375 to 0.09375
- last_down: bfloat16 [12288, 4096], P('tp', 'kv'), may hold values from -0.078125 to 0.078125
Outputs:
- result: bfloat16 [256, 4096], P(None, ('kv', 'tp'))
- new_memory: float32 [256, 16, 256, 128], P('kv', 'tp')
- new_normalizer: float32 [256, 16, 128], P('kv', 'tp')
- new_stabilizer: float32 [256, 16], P('kv', 'tp')
The draws below stay inside these ranges and needn't reach their ends.
All inputs are finite; a program needn't handle non-finite values.
Results may differ from the reference program's by a relative error of at most 0.025.
Values may be sent and summed in bfloat16 or wider, within the bound.
A program may use at most 64 MiB of HBM per device.

```python
import jax
import jax.numpy as jnp
from jax import lax

D = 4096
FF = 12288
HEADS = 16
DK = 128
DV = 256
BATCH = 256


def strengthened(entries, own_key, source, target, blocks, factor):
    def block_of(dim):
        return (jnp.arange(entries.shape[dim]) // (entries.shape[dim] // blocks)).reshape((-1,) + (1,) * (entries.ndim - 1 - dim))

    first = jax.random.permutation(own_key, blocks)[block_of(target)]
    other_side = (block_of(target) + blocks // 2) % blocks
    return jnp.where((block_of(source) == first) | (block_of(source) == other_side), factor * entries, entries)


def block_scale(key, extent, cuts, smallest, top_value):
    def one(axis_at, blocks):
        heights = jax.random.uniform(jax.random.fold_in(jax.random.fold_in(key, 6), axis_at), (blocks,), jnp.float32, smallest / len(cuts), top_value / len(cuts))
        return jnp.repeat(jnp.exp(heights), extent[axis_at] // blocks).reshape((-1,) + (1,) * (len(extent) - axis_at - 1))

    loudness = one(*cuts[0])
    for cut in cuts[1:]:
        loudness = loudness * one(*cut)
    return loudness


def normal_values(own_key, shape, deviation, most, pieces=(), held_as=jnp.bfloat16):
    level = block_scale(own_key, shape, pieces, -0.22, 0.18) if pieces else 1.0
    drawn = jax.random.normal(own_key, shape, jnp.float32) * deviation * level
    return jnp.minimum(jnp.maximum(drawn, -most), most).astype(held_as)


def gaussian_with(stream_key, dims, spread, reach, cuts, heavy, dtype=jnp.bfloat16):
    values = spread * jax.random.normal(stream_key, dims, jnp.float32)
    if cuts:
        values = values * block_scale(stream_key, dims, cuts, -0.22, 0.18)
    return jnp.clip(strengthened(values, jax.random.fold_in(stream_key, 3), *heavy), -reach, reach).astype(dtype)


def setup_inputs(seed: int = 0) -> dict:
    arg_keys = jax.random.split(jax.random.key(seed), 21)
    tokens = normal_values(arg_keys[0], (BATCH, D), 1.0, 6.0, ((1, 256),))
    memory = normal_values(arg_keys[1], (BATCH, HEADS, DV, DK), 1.0, 6.0, ((0, 16), (1, 16)), jnp.float32)
    normalizer = normal_values(arg_keys[2], (BATCH, HEADS, DK), 1.0, 6.0, ((0, 16), (1, 16)), jnp.float32)
    stabilizer = normal_values(arg_keys[3], (BATCH, HEADS), 1.0, 4.0, ((0, 16), (1, 16)), jnp.float32)
    first_gain = jnp.clip(1.0 + 0.18 * jax.random.normal(arg_keys[4], (D,), jnp.float32), 0.1, 1.9)
    first_gate = normal_values(arg_keys[5], (D, FF), D ** -0.5, 0.09375, ((0, 16), (1, 16)))
    first_up = normal_values(arg_keys[6], (D, FF), D ** -0.5, 0.09375, ((0, 16), (1, 16)))
    first_down = gaussian_with(arg_keys[7], (FF, D), FF ** -0.5, 0.078125, ((0, 16), (1, 16)), (0, 1, 16, 2.0))
    mixer_gain = jnp.clip(1.0 + 0.18 * jax.random.normal(arg_keys[8], (D,), jnp.float32), 0.1, 1.9)
    query_weight = normal_values(arg_keys[9], (D, HEADS * DK), D ** -0.5, 0.09375, ((1, 16),))
    key_weight = normal_values(arg_keys[10], (D, HEADS * DK), D ** -0.5, 0.09375, ((1, 16),))
    value_weight = normal_values(arg_keys[11], (D, HEADS * DV), D ** -0.5, 0.09375, ((1, 16),))
    input_weight = normal_values(arg_keys[12], (D, HEADS), D ** -0.5, 0.09375)
    forget_weight = normal_values(arg_keys[13], (D, HEADS), D ** -0.5, 0.09375)
    forget_bias = jnp.clip(-2.0 + 6.0 * jax.random.uniform(arg_keys[14], (HEADS,), jnp.float32) ** block_scale(arg_keys[14], (HEADS,), ((0, 16),), -0.2, 0.2), -2.0, 4.0)
    output_weight = normal_values(arg_keys[15], (HEADS * DV, D), (HEADS * DV) ** -0.5, 0.09375, ((0, 16),))
    last_gain = jnp.clip(1.0 + 0.18 * jax.random.normal(arg_keys[16], (D,), jnp.float32), 0.1, 1.9)
    last_gate = normal_values(arg_keys[17], (D, FF), D ** -0.5, 0.09375, ((0, 16), (1, 16)))
    last_up = normal_values(arg_keys[18], (D, FF), D ** -0.5, 0.09375, ((0, 16), (1, 16)))
    last_down = gaussian_with(arg_keys[19], (FF, D), FF ** -0.5, 0.078125, ((0, 16), (1, 16)), (0, 1, 16, 2.0))
    return {"tokens": tokens, "memory": memory, "normalizer": normalizer, "stabilizer": stabilizer, "first_gain": first_gain, "first_gate": first_gate, "first_up": first_up, "first_down": first_down, "mixer_gain": mixer_gain, "query_weight": query_weight, "key_weight": key_weight, "value_weight": value_weight, "input_weight": input_weight, "forget_weight": forget_weight, "forget_bias": forget_bias, "output_weight": output_weight, "last_gain": last_gain, "last_gate": last_gate, "last_up": last_up, "last_down": last_down}


EPS = 1e-06

def norm_scale(stream):
    values = stream.astype(jnp.float32)
    return lax.rsqrt(lax.optimization_barrier(jnp.mean(values * values, axis=-1, keepdims=True)) + EPS)

def gated_mlp(stream, gain, w_gate, w_up, w_down):
    scale = norm_scale(stream)
    scaled = (stream.astype(jnp.float32) * gain).astype(jnp.bfloat16)
    gate = scale * jnp.dot(scaled, w_gate, preferred_element_type=jnp.float32)
    up = scale * jnp.dot(scaled, w_up, preferred_element_type=jnp.float32)
    hidden = (jax.nn.silu(gate) * up).astype(jnp.bfloat16)
    return jnp.dot(hidden, w_down, preferred_element_type=jnp.float32)

def reference(tokens, memory, normalizer, stabilizer, first_gain, first_gate, first_up, first_down, mixer_gain, query_weight, key_weight, value_weight, input_weight, forget_weight, forget_bias, output_weight, last_gain, last_gate, last_up, last_down):
    f32 = jnp.float32
    first_sum = gated_mlp(tokens, first_gain, first_gate, first_up, first_down)
    stream_one = (tokens.astype(f32) + 0.5 * first_sum).astype(jnp.bfloat16)
    batch = tokens.shape[0]
    scale = norm_scale(stream_one)
    cell_in = (stream_one.astype(f32) * mixer_gain).astype(jnp.bfloat16)
    query = (scale * jnp.dot(cell_in, query_weight, preferred_element_type=f32) * DK ** (-0.5)).reshape(batch, HEADS, DK)
    key = (scale * jnp.dot(cell_in, key_weight, preferred_element_type=f32)).reshape(batch, HEADS, DK)
    value = (scale * jnp.dot(cell_in, value_weight, preferred_element_type=f32)).reshape(batch, HEADS, DV)
    input_pre = scale * jnp.dot(cell_in, input_weight, preferred_element_type=f32)
    log_forget = jax.nn.log_sigmoid(scale * jnp.dot(cell_in, forget_weight, preferred_element_type=f32) + forget_bias)
    carried = log_forget + stabilizer
    new_stabilizer = jnp.maximum(carried, input_pre)
    keep = jnp.exp(carried - new_stabilizer)
    admit = jnp.exp(input_pre - new_stabilizer)
    recalled = jnp.einsum('bhvd,bhd->bhv', memory, query, precision=lax.Precision.HIGHEST)
    match = lax.optimization_barrier(jnp.sum(query * key, axis=-1))
    numer = keep[..., None] * recalled + (admit * match)[..., None] * value
    denom = keep * lax.optimization_barrier(jnp.sum(normalizer * query, axis=-1)) + admit * match
    cell_out = (numer / jnp.maximum(jnp.abs(denom), 1.0)[..., None]).reshape(batch, HEADS * DV).astype(jnp.bfloat16)
    new_memory = keep[..., None, None] * memory + admit[..., None, None] * value[..., :, None] * key[..., None, :]
    new_normalizer = keep[..., None] * normalizer + admit[..., None] * key
    mixed = jnp.dot(cell_out, output_weight, preferred_element_type=f32)
    stream_two = (stream_one.astype(f32) + mixed).astype(jnp.bfloat16)
    last_sum = gated_mlp(stream_two, last_gain, last_gate, last_up, last_down)
    result = (stream_two.astype(f32) + 0.5 * last_sum).astype(jnp.bfloat16)
    return (result, new_memory, new_normalizer, new_stabilizer)
```

```python
import jax
import jax.numpy as jnp
from jax import lax
from jax.experimental import pallas as pl
from jax.experimental.pallas import tpu as pltpu
from jax.sharding import PartitionSpec as P

EPS = 1e-06
MESH = pl.DeviceIdType.MESH
F32 = jnp.float32
BF16 = jnp.bfloat16
KV_OFFSETS = (
    (2, 2), (1, 2), (2, 1), (3, 2), (2, 3), (1, 1), (3, 3), (1, 3),
    (3, 1), (0, 2), (2, 0), (0, 1), (1, 0), (0, 3), (3, 0),
)
TP_OFFSETS = (
    (4, 0), (4, 1), (3, 0), (5, 0), (3, 1), (5, 1), (2, 0), (6, 0),
    (2, 1), (6, 1), (1, 0), (7, 0), (1, 1), (7, 1), (0, 1),
)


def nt(a, b):
    return lax.dot_general(a, b, (((1,), (1,)), ((), ())), preferred_element_type=F32)


def nn(a, b):
    return jnp.dot(a, b, preferred_element_type=F32)


def kernel(
    tok_hbm, mem_hbm, nrm_hbm, stab_hbm, g1_hbm, wg1_hbm, wu1_hbm, wd1_hbm, g2_hbm,
    wq_hbm, wk_hbm, wv_hbm, wi_hbm, wf_hbm, fb_hbm, wo_hbm, g3_hbm, wg3_hbm, wu3_hbm, wd3_hbm,
    res_ref, newmem_hbm, newnrm_ref, newstab_ref,
    mem, memb, memout, nrm, stab, g1, wg1, wu1, wd1, g2, wq, wk, wv, wif, fb, wo, g3, wg3, wu3, wd3,
    recv1, blk, send2, recv2, hid, recv3, send4, recv4, send5, recv5, cell, send6, recv6,
    send7, recv7, blk_t, send8, recv8, hid2, recv9, wd3t, send10, recv10,
    lsem, ssem, rsem, osem,
):
    kv = lax.axis_index("kv")
    tp = lax.axis_index("tp")
    y, x = kv // 4, kv % 4
    z, core = tp // 2, tp % 2
    kv_peers = [lax.rem(y + dy, 4) * 4 + lax.rem(x + dx, 4) for dy, dx in KV_OFFSETS]
    tp_peers = [lax.rem(z + dz, 8) * 2 + lax.rem(core + dc, 2) for dz, dc in TP_OFFSETS]
    diag = kv == tp

    pairs = [
        (tok_hbm, recv1.at[tp]), (wg1_hbm, wg1), (wu1_hbm, wu1), (g1_hbm, g1), (wd1_hbm, wd1),
        (wq_hbm, wq), (wk_hbm, wk), (wv_hbm, wv), (wi_hbm, wif.at[pl.ds(0, 16)]),
        (wf_hbm, wif.at[pl.ds(16, 16)]), (g2_hbm, g2), (mem_hbm, mem), (nrm_hbm, nrm),
        (stab_hbm, stab), (fb_hbm, fb), (wo_hbm, wo), (g3_hbm, g3), (wg3_hbm, wg3),
        (wu3_hbm, wu3), (wd3_hbm, wd3),
    ]
    loads = [pltpu.make_async_copy(s, d, lsem.at[i]) for i, (s, d) in enumerate(pairs)]
    for c in loads:
        c.start()
    (ld_tok, ld_wg1, ld_wu1, ld_g1, ld_wd1, ld_wq, ld_wk, ld_wv, ld_wi, ld_wf, ld_g2, ld_mem,
     ld_nrm, ld_stab, ld_fb, ld_wo, ld_g3, ld_wg3, ld_wu3, ld_wd3) = loads

    barrier = pltpu.get_barrier_semaphore()

    def greet(k, t):
        pl.semaphore_signal(barrier, inc=1, device_id=(k, t), device_id_type=MESH)

    for k in kv_peers:
        greet(k, tp)
    for t in tp_peers:
        greet(kv, t)

    @pl.loop(0, 16)
    def _(j):
        @pl.when(jnp.logical_not(jnp.logical_and(diag, j == tp)))
        def _():
            greet(tp, j)
            greet(j, kv)

    pl.semaphore_wait(barrier, jnp.where(diag, 60, 62))
    ld_tok.wait()

    def send(src, dst, phase, k, t):
        pltpu.make_async_remote_copy(
            src_ref=src, dst_ref=dst, send_sem=ssem.at[phase], recv_sem=rsem.at[phase],
            device_id=(k, t), device_id_type=MESH,
        ).start()

    def arrived(buf, phase, count=15):
        part = buf.at[pl.ds(0, count)]
        pltpu.make_async_copy(part, part, rsem.at[phase]).wait()

    def sent(buf, phase, count=15):
        part = buf.at[pl.ds(0, count)]
        pltpu.make_async_copy(part, part, ssem.at[phase]).wait()

    def gain_row(g, c):
        return jnp.concatenate([g[pl.ds(2 * c, 1), :], g[pl.ds(2 * c + 1, 1), :]], axis=1)

    for t in tp_peers:
        send(recv1.at[tp], recv1.at[tp], 0, kv, t)

    arrived(recv1, 0)
    blk[...] = recv1[...].reshape(256, 256).T

    def gate_up(block, gain, wg, wu, out, into, phase):
        vals = block.astype(F32)
        scaled = (vals * gain).astype(BF16)
        sq = jnp.sum(vals * vals, axis=1, keepdims=True)
        out[:, :, pl.ds(1536, 128)] = jnp.broadcast_to(sq, (256, 128)).astype(BF16).reshape(16, 16, 128)
        for n in range(3):
            cols = pl.ds(n * 256, 256)
            out[:, :, cols] = nn(scaled, wg[:, cols]).astype(BF16).reshape(16, 16, 256)
            out[:, :, pl.ds(768 + n * 256, 256)] = nn(scaled, wu[:, cols]).astype(BF16).reshape(16, 16, 256)
        for k in kv_peers:
            send(out.at[k], into.at[kv], phase, k, tp)
        into[pl.ds(kv, 1)] = out[pl.ds(kv, 1)]

    def hidden(into, phase, out, gathered, next_phase):
        arrived(into, phase)
        scale = lax.rsqrt(jnp.sum(into[:, :, pl.ds(1536, 128)].astype(F32), axis=0)[:, :1] / 4096 + EPS)
        gate = scale * jnp.sum(into[:, :, pl.ds(0, 768)].astype(F32), axis=0)
        up = scale * jnp.sum(into[:, :, pl.ds(768, 768)].astype(F32), axis=0)
        h = (gate / (1.0 + jnp.exp(-gate)) * up).astype(BF16)
        gathered[pl.ds(kv, 1)] = h[None]
        for k in kv_peers:
            send(gathered.at[kv], gathered.at[kv], next_phase, k, tp)

    def to_group(buf, into, phase):
        @pl.loop(0, 16)
        def _(j):
            @pl.when(jnp.logical_not(jnp.logical_and(diag, j == tp)))
            def _():
                send(buf, into.at[kv], phase, tp, j)

        @pl.when(diag)
        def _():
            into[pl.ds(kv, 1)] = buf[...][None]

    def from_group(buf, wait, phase):
        @pl.when(diag)
        def _():
            wait(buf, phase, 15)

        @pl.when(jnp.logical_not(diag))
        def _():
            wait(buf, phase, 16)

    ld_wg1.wait()
    ld_wu1.wait()
    ld_g1.wait()
    gate_up(blk[...], gain_row(g1, kv), wg1, wu1, send2, recv2, 1)
    ld_mem.wait()
    memb[...] = mem[...].astype(BF16)
    hidden(recv2, 1, hid, recv3, 2)
    ld_wd1.wait()
    arrived(recv3, 2)

    send4[...] = nn(recv3[...].reshape(256, 768), wd1[...]).astype(BF16).reshape(16, 16, 256)
    for t in tp_peers:
        send(send4.at[t], recv4.at[tp], 3, kv, t)
    recv4[pl.ds(tp, 1)] = send4[pl.ds(tp, 1)]
    for c in (ld_wq, ld_wk, ld_wv, ld_wi, ld_wf, ld_g2, ld_nrm, ld_stab, ld_fb):
        c.wait()
    arrived(recv4, 3)
    first = jnp.sum(recv4[...].astype(F32), axis=0)
    rows = pl.ds(pl.multiple_of(tp * 16, 16), 16)
    send5[...] = (blk[rows, :].astype(F32) + 0.5 * first).astype(BF16)

    to_group(send5, recv5, 4)
    from_group(recv5, arrived, 4)

    sq = jnp.zeros((16, 256), F32)
    for c in range(16):
        v = recv5[c].astype(F32)
        sq = sq + v * v
        cell[:, pl.ds(c * 256, 256)] = (v * gain_row(g2, c)).astype(BF16)
    scale = lax.rsqrt(jnp.sum(sq, axis=1, keepdims=True) / 4096 + EPS)
    query = scale * nn(cell[...], wq[...]) * 128 ** (-0.5)
    key = scale * nn(cell[...], wk[...])
    value = scale * nn(cell[...], wv[...])
    gates = nt(cell[...], wif[...])
    lane32 = lax.broadcasted_iota(jnp.int32, (16, 32), 1)
    input_pre = scale * jnp.sum(jnp.where(lane32 == tp, gates, 0.0), axis=1, keepdims=True)
    pre = scale * jnp.sum(jnp.where(lane32 == tp + 16, gates, 0.0), axis=1, keepdims=True) + fb[...]
    log_forget = jnp.minimum(pre, 0.0) - jnp.log1p(jnp.exp(-jnp.abs(pre)))
    eye = lax.broadcasted_iota(jnp.int32, (16, 16), 0) == lax.broadcasted_iota(jnp.int32, (16, 16), 1)
    old_stab = jnp.sum(jnp.where(eye, jnp.broadcast_to(stab[...], (16, 16)), 0.0), axis=1, keepdims=True)
    carried = log_forget + old_stab
    new_stab = jnp.maximum(carried, input_pre)
    keep = jnp.exp(carried - new_stab)
    admit = jnp.exp(input_pre - new_stab)
    match = jnp.sum(query * key, axis=1, keepdims=True)
    denom = keep * jnp.sum(nrm[...] * query, axis=1, keepdims=True) + admit * match
    qb = query.astype(BF16)
    row256 = lax.broadcasted_iota(jnp.int32, (16, 256), 0)
    recalled = jnp.zeros((16, 256), F32)
    for b in range(16):
        recalled = jnp.where(row256 == b, nt(qb, memb[b]), recalled)
    numer = keep * recalled + (admit * match) * value
    cell_out = (numer / jnp.maximum(jnp.abs(denom), 1.0)).astype(BF16)

    ld_wo.wait()
    for c in range(16):
        send6[c] = nn(cell_out, wo[:, pl.ds(c * 256, 256)]).astype(BF16)
    for t in tp_peers:
        send(send6.at[t], recv6.at[tp], 5, kv, t)
    recv6[pl.ds(tp, 1)] = send6[pl.ds(tp, 1)]

    newnrm_ref[...] = keep * nrm[...] + admit * key
    newstab_ref[...] = jnp.sum(jnp.where(eye, jnp.broadcast_to(new_stab, (16, 16)), 0.0), axis=0, keepdims=True)
    added = admit * key
    vh = value.astype(BF16)
    vl = (value - vh.astype(F32)).astype(BF16)
    vt = jnp.concatenate([vh.astype(F32), vl.astype(F32), vh.astype(F32)], axis=0).T.astype(BF16)
    row128 = lax.broadcasted_iota(jnp.int32, (16, 128), 0)
    kh = added.astype(BF16).astype(F32)
    kl = added - kh
    for b in range(16):
        khb = jnp.where(row128 == b, kh, 0.0)
        klb = jnp.where(row128 == b, kl, 0.0)
        outer = nn(vt, jnp.concatenate([khb, khb, klb], axis=0).astype(BF16))
        kb = jnp.sum(jnp.where(row128[:, :1] == b, keep, 0.0), axis=0, keepdims=True)
        memout[b] = kb * mem[b] + outer
    put = pltpu.make_async_copy(memout, newmem_hbm, osem)
    put.start()

    arrived(recv6, 5)
    mixed = jnp.sum(recv6[...].astype(F32), axis=0)
    send7[...] = (recv5[pl.ds(tp, 1)][0].astype(F32) + mixed).astype(BF16)

    to_group(send7, recv7, 6)
    for c in (ld_wg3, ld_wu3, ld_g3, ld_wd3):
        c.wait()
    wd3t[...] = wd3[...].T
    from_group(recv7, arrived, 6)

    block = recv7[...].reshape(256, 256)
    gate_up(block, gain_row(g3, kv), wg3, wu3, send8, recv8, 7)
    blk_t[...] = block.T
    hidden(recv8, 7, hid2, recv9, 8)
    arrived(recv9, 8)

    send10[...] = nt(wd3t[...], recv9[...].reshape(256, 768)).astype(BF16).reshape(16, 16, 256)
    for t in tp_peers:
        send(send10.at[t], recv10.at[tp], 9, kv, t)
    recv10[pl.ds(tp, 1)] = send10[pl.ds(tp, 1)]
    arrived(recv10, 9)
    last = jnp.sum(recv10[...].astype(F32), axis=0)
    res_ref[...] = (blk_t[rows, :].astype(F32) + 0.5 * last).astype(BF16)

    sent(recv1, 0)
    sent(send2, 1)
    sent(recv3, 2)
    sent(send4, 3)
    from_group(recv5, sent, 4)
    sent(send6, 5)
    from_group(recv7, sent, 6)
    sent(send8, 7)
    sent(recv9, 8)
    sent(send10, 9)
    put.wait()


def layer(
    tokens, memory, normalizer, stabilizer, first_gain, first_gate, first_up, first_down, mixer_gain,
    query_weight, key_weight, value_weight, input_weight, forget_weight, forget_bias, output_weight,
    last_gain, last_gate, last_up, last_down,
):
    any_ = pl.BlockSpec(memory_space=pl.ANY)
    vmem = pl.BlockSpec(memory_space=pltpu.VMEM)
    b = lambda *s: pltpu.VMEM(s, BF16)
    f = lambda *s: pltpu.VMEM(s, F32)
    scratch = [
        f(16, 256, 128), b(16, 256, 128), f(16, 256, 128), f(16, 128), f(1, 16),
        f(32, 128), b(256, 768), b(256, 768), b(768, 256), f(32, 128),
        b(4096, 128), b(4096, 128), b(4096, 256), b(32, 4096), f(1, 1), b(256, 4096),
        f(32, 128), b(256, 768), b(256, 768), b(768, 256),
        b(16, 16, 256), b(256, 256), b(16, 16, 1664), b(16, 16, 1664), b(16, 768), b(16, 16, 768),
        b(16, 16, 256), b(16, 16, 256), b(16, 256), b(16, 16, 256), b(16, 4096),
        b(16, 16, 256), b(16, 16, 256), b(16, 256), b(16, 16, 256), b(256, 256),
        b(16, 16, 1664), b(16, 16, 1664), b(16, 768), b(16, 16, 768), b(256, 768),
        b(16, 16, 256), b(16, 16, 256),
        pltpu.SemaphoreType.DMA((20,)), pltpu.SemaphoreType.DMA((10,)),
        pltpu.SemaphoreType.DMA((10,)), pltpu.SemaphoreType.DMA,
    ]
    res, new_mem, new_nrm, new_stab = pl.pallas_call(
        kernel,
        out_shape=(
            jax.ShapeDtypeStruct((16, 256), BF16),
            jax.ShapeDtypeStruct((16, 256, 128), F32),
            jax.ShapeDtypeStruct((16, 128), F32),
            jax.ShapeDtypeStruct((1, 16), F32),
        ),
        in_specs=[any_] * 20,
        out_specs=(vmem, any_, vmem, vmem),
        scratch_shapes=scratch,
        compiler_params=pltpu.CompilerParams(
            collective_id=0, has_side_effects=True, vmem_limit_bytes=60 * 1024 * 1024
        ),
        name="layer",
    )(
        tokens.T, memory.reshape(16, 256, 128), normalizer.reshape(16, 128), stabilizer.reshape(1, 16),
        first_gain.reshape(32, 128), first_gate, first_up, first_down, mixer_gain.reshape(32, 128),
        query_weight, key_weight, value_weight, input_weight.T, forget_weight.T,
        forget_bias.reshape(1, 1), output_weight, last_gain.reshape(32, 128), last_gate, last_up, last_down,
    )
    return res.T, new_mem.reshape(16, 1, 256, 128), new_nrm.reshape(16, 1, 128), new_stab.reshape(16, 1)


def solution(mesh):
    in_specs = (
        P(None, ("kv", "tp")), P("kv", "tp", None, None), P("kv", "tp", None), P("kv", "tp"), P(),
        P("kv", "tp"), P("kv", "tp"), P("tp", "kv"), P(), P(None, "tp"), P(None, "tp"), P(None, "tp"),
        P(), P(), P("tp"), P("tp", None), P(), P("kv", "tp"), P("kv", "tp"), P("tp", "kv"),
    )
    out_specs = (P(None, ("kv", "tp")), P("kv", "tp", None, None), P("kv", "tp", None), P("kv", "tp"))
    return jax.shard_map(layer, mesh=mesh, in_specs=in_specs, out_specs=out_specs, check_vma=False)
```

```python
import jax
import jax.numpy as jnp
from jax import lax
from jax.experimental import pallas as pl
from jax.experimental.pallas import tpu as pltpu
from jax.sharding import PartitionSpec as P

EPS = 1e-06
MESH = pl.DeviceIdType.MESH
F32 = jnp.float32
BF16 = jnp.bfloat16
KV_OFFSETS = (
    (2, 2), (1, 2), (2, 1), (3, 2), (2, 3), (1, 1), (3, 3), (1, 3),
    (3, 1), (0, 2), (2, 0), (0, 1), (1, 0), (0, 3), (3, 0),
)
TP_OFFSETS = (
    (4, 0), (4, 1), (3, 0), (5, 0), (3, 1), (5, 1), (2, 0), (6, 0),
    (2, 1), (6, 1), (1, 0), (7, 0), (1, 1), (7, 1), (0, 1),
)
WIDE = 1664


def nt(a, b):
    return lax.dot_general(a, b, (((1,), (1,)), ((), ())), preferred_element_type=F32)


def nn(a, b):
    return jnp.dot(a, b, preferred_element_type=F32)


def kernel(
    tok_hbm, mem_hbm, nrm_hbm, stab_hbm, g1_hbm, wg1_hbm, wu1_hbm, wd1_hbm, g2_hbm,
    wq_hbm, wk_hbm, wv_hbm, wi_hbm, wf_hbm, fb_hbm, wo_hbm, g3_hbm, wg3_hbm, wu3_hbm, wd3_hbm,
    res_ref, memout, newnrm_ref, newstab_ref,
    tok, mem, memb, nrm, stab, g1, wg1, wu1, wd1, g2, wq, wk, wv, wif, fb, wo, g3, wg3, wu3, wd3,
    recv1, blk, send2, recv2, send2b, recv2b, recv3, send4, recv4, send5, recv5, cell, send6, recv6,
    send7, recv7, blk_t, send8, recv8, send8b, recv8b, recv9, wd3t, send10, recv10,
    lsem, ssem, rsem,
):
    kv = lax.axis_index("kv")
    tp = lax.axis_index("tp")
    y, x = kv // 4, kv % 4
    z, core = tp // 2, tp % 2
    kv_peers = [lax.rem(y + dy, 4) * 4 + lax.rem(x + dx, 4) for dy, dx in KV_OFFSETS]
    tp_peers = [lax.rem(z + dz, 8) * 2 + lax.rem(core + dc, 2) for dz, dc in TP_OFFSETS]
    diag = kv == tp
    a_me = jnp.where(core == 0, x, y)
    b_me = jnp.where(core == 0, y, x)
    g_me = a_me * 4 + b_me
    a_peers = [lax.rem(a_me + d, 4) for d in (2, 1, 3)]
    b_peers = [lax.rem(b_me + d, 4) for d in (2, 1, 3)]

    def at(a, b):
        return jnp.where(core == 0, b * 4 + a, a * 4 + b)

    pairs = [
        (tok_hbm, tok), (wg1_hbm, wg1), (wu1_hbm, wu1), (g1_hbm, g1), (wd1_hbm, wd1),
        (wq_hbm, wq), (wk_hbm, wk), (wv_hbm, wv), (wi_hbm, wif.at[pl.ds(0, 16)]),
        (wf_hbm, wif.at[pl.ds(16, 16)]), (g2_hbm, g2), (mem_hbm, mem), (nrm_hbm, nrm),
        (stab_hbm, stab), (fb_hbm, fb), (wo_hbm, wo), (g3_hbm, g3), (wg3_hbm, wg3),
        (wu3_hbm, wu3), (wd3_hbm, wd3),
    ]
    loads = [pltpu.make_async_copy(s, d, lsem.at[i]) for i, (s, d) in enumerate(pairs)]
    for c in loads:
        c.start()
    (ld_tok, ld_wg1, ld_wu1, ld_g1, ld_wd1, ld_wq, ld_wk, ld_wv, ld_wi, ld_wf, ld_g2, ld_mem,
     ld_nrm, ld_stab, ld_fb, ld_wo, ld_g3, ld_wg3, ld_wu3, ld_wd3) = loads

    barrier = pltpu.get_barrier_semaphore()
    for k in kv_peers:
        pl.semaphore_signal(barrier, inc=1, device_id=(k, tp), device_id_type=MESH)
    for t in tp_peers:
        pl.semaphore_signal(barrier, inc=1, device_id=(kv, t), device_id_type=MESH)

    def send(src, dst, sem, k, t):
        pltpu.make_async_remote_copy(
            src_ref=src, dst_ref=dst, send_sem=ssem.at[sem], recv_sem=rsem.at[sem],
            device_id=(k, t), device_id_type=MESH,
        ).start()

    def arrived(buf, sem, count):
        part = buf.at[pl.ds(0, count)]
        pltpu.make_async_copy(part, part, rsem.at[sem]).wait()

    def sent(buf, sem, count):
        part = buf.at[pl.ds(0, count)]
        pltpu.make_async_copy(part, part, ssem.at[sem]).wait()

    def gain_row(g, c):
        return jnp.concatenate([g[pl.ds(2 * c, 1), :], g[pl.ds(2 * c + 1, 1), :]], axis=1)

    spot = lax.broadcasted_iota(jnp.int32, (256, 256), 1)
    seq = lax.broadcasted_iota(jnp.int32, (256, 256), 0)
    spot_row = ((spot % 128) // 8) * 16 + (spot // 128) * 8 + spot % 8
    order = jnp.where(seq == spot_row, 1.0, 0.0).astype(BF16)
    ld_tok.wait()
    ordered = nn(tok[...], order).astype(BF16)
    for h in range(2):
        recv1[h, pl.ds(tp, 1)] = ordered[:, h * 128 : h * 128 + 128][None]
    pl.semaphore_wait(barrier, 30)

    for h in range(2):
        for t in tp_peers:
            send(recv1.at[h, tp], recv1.at[h, tp], h, kv, t)

    def gate_up(h, block, gain, wg, wu, out, into, sem):
        vals = block.astype(F32)
        scaled = (vals * gain).astype(BF16)
        sq = jnp.sum(vals * vals, axis=1, keepdims=True)
        out[h, :, :, pl.ds(1536, 128)] = jnp.broadcast_to(sq, (128, 128)).astype(BF16).reshape(4, 32, 128)
        for n in range(3):
            cols = pl.ds(n * 256, 256)
            out[h, :, :, cols] = nn(scaled, wg[:, cols]).astype(BF16).reshape(4, 32, 256)
            out[h, :, :, pl.ds(768 + n * 256, 256)] = nn(scaled, wu[:, cols]).astype(BF16).reshape(4, 32, 256)
        for a in a_peers:
            send(out.at[h, a], into.at[h, a_me], sem, at(a, b_me), tp)
        into[h, pl.ds(a_me, 1)] = out[h, pl.ds(a_me, 1)]

    def second_sum(h, into, sem, out, next_into, next_sem):
        arrived(into.at[h], sem, 3)
        for n in range(0, WIDE, 128):
            cols = pl.ds(n, 128)
            total = jnp.sum(into[h, :, :, cols].astype(F32), axis=0)
            out[h, :, :, cols] = total.reshape(4, 8, 128).astype(BF16)
        for b in b_peers:
            send(out.at[h, b], next_into.at[h, b_me], next_sem, at(a_me, b), tp)
        next_into[h, pl.ds(b_me, 1)] = out[h, pl.ds(b_me, 1)]

    def hidden(h, into, sem, gathered, next_sem):
        arrived(into.at[h], sem, 3)
        total = jnp.sum(into[h].astype(F32), axis=0)
        scale = lax.rsqrt(total[:, 1536:1537] / 4096 + EPS)
        gate = scale * total[:, :768]
        up = scale * total[:, 768:1536]
        gathered[h, pl.ds(g_me, 1)] = (gate / (1.0 + jnp.exp(-gate)) * up).astype(BF16)[None]
        for k in kv_peers:
            send(gathered.at[h, g_me], gathered.at[h, g_me], next_sem, k, tp)

    def to_group(buf, into, sem):
        @pl.loop(0, 16)
        def _(j):
            @pl.when(jnp.logical_not(jnp.logical_and(diag, j == tp)))
            def _():
                send(buf, into.at[kv], sem, tp, j)

        @pl.when(diag)
        def _():
            into[pl.ds(kv, 1)] = buf[...][None]

    def from_group(buf, wait, sem):
        @pl.when(diag)
        def _():
            wait(buf, sem, 15)

        @pl.when(jnp.logical_not(diag))
        def _():
            wait(buf, sem, 16)

    gain = None
    for h in range(2):
        arrived(recv1.at[h], h, 15)
        block = recv1[h].reshape(256, 128).T
        blk[h] = block.reshape(16, 8, 256)
        if h == 0:
            ld_wg1.wait()
            ld_wu1.wait()
            ld_g1.wait()
            gain = gain_row(g1, kv)
        gate_up(h, block, gain, wg1, wu1, send2, recv2, 2 + h)
    for h in range(2):
        second_sum(h, recv2, 2 + h, send2b, recv2b, 4 + h)
    for h in range(2):
        hidden(h, recv2b, 4 + h, recv3, 6 + h)

    ld_wd1.wait()
    for h in range(2):
        arrived(recv3.at[h], 6 + h, 15)
        send4[h] = nn(recv3[h].reshape(128, 768), wd1[...]).astype(BF16).reshape(16, 8, 256)
        for t in tp_peers:
            send(send4.at[h, t], recv4.at[h, tp], 8 + h, kv, t)
        recv4[h, pl.ds(tp, 1)] = send4[h, pl.ds(tp, 1)]
    for c in (ld_wq, ld_wk, ld_wv, ld_wi, ld_wf, ld_g2, ld_nrm, ld_stab, ld_fb, ld_mem, ld_wo):
        c.wait()
    memb[...] = mem[...].astype(BF16)

    for h in range(2):
        arrived(recv4.at[h], 8 + h, 15)
        first = jnp.sum(recv4[h].astype(F32), axis=0)
        send5[h] = (blk[h, pl.ds(tp, 1)][0].astype(F32) + 0.5 * first).astype(BF16)
        to_group(send5.at[h], recv5.at[h], 10 + h)
    for h in range(2):
        from_group(recv5.at[h], arrived, 10 + h)

    sq = jnp.zeros((16, 256), F32)
    for c in range(16):
        v = jnp.concatenate([recv5[0, c].astype(F32), recv5[1, c].astype(F32)], axis=0)
        sq = sq + v * v
        cell[:, pl.ds(c * 256, 256)] = (v * gain_row(g2, c)).astype(BF16)
    scale = lax.rsqrt(jnp.sum(sq, axis=1, keepdims=True) / 4096 + EPS)
    query = scale * nn(cell[...], wq[...]) * 128 ** (-0.5)
    key = scale * nn(cell[...], wk[...])
    value = scale * nn(cell[...], wv[...])
    gates = nt(cell[...], wif[...])
    lane32 = lax.broadcasted_iota(jnp.int32, (16, 32), 1)
    input_pre = scale * jnp.sum(jnp.where(lane32 == tp, gates, 0.0), axis=1, keepdims=True)
    pre = scale * jnp.sum(jnp.where(lane32 == tp + 16, gates, 0.0), axis=1, keepdims=True) + fb[...]
    log_forget = jnp.minimum(pre, 0.0) - jnp.log1p(jnp.exp(-jnp.abs(pre)))
    eye = lax.broadcasted_iota(jnp.int32, (16, 16), 0) == lax.broadcasted_iota(jnp.int32, (16, 16), 1)
    old_stab = jnp.sum(jnp.where(eye, jnp.broadcast_to(stab[...], (16, 16)), 0.0), axis=1, keepdims=True)
    carried = log_forget + old_stab
    new_stab = jnp.maximum(carried, input_pre)
    keep = jnp.exp(carried - new_stab)
    admit = jnp.exp(input_pre - new_stab)
    match = jnp.sum(query * key, axis=1, keepdims=True)
    denom = keep * jnp.sum(nrm[...] * query, axis=1, keepdims=True) + admit * match
    qb = query.astype(BF16)
    row256 = lax.broadcasted_iota(jnp.int32, (16, 256), 0)
    recalled = jnp.zeros((16, 256), F32)
    for b in range(16):
        recalled = jnp.where(row256 == b, nt(qb, memb[b]), recalled)
    numer = keep * recalled + (admit * match) * value
    cell_out = (numer / jnp.maximum(jnp.abs(denom), 1.0)).astype(BF16)

    for c in range(16):
        send6[:, c] = nn(cell_out, wo[:, pl.ds(c * 256, 256)]).astype(BF16).reshape(2, 8, 256)
    for h in range(2):
        for t in tp_peers:
            send(send6.at[h, t], recv6.at[h, tp], 12 + h, kv, t)
        recv6[h, pl.ds(tp, 1)] = send6[h, pl.ds(tp, 1)]

    for c in (ld_wg3, ld_wu3, ld_g3, ld_wd3):
        c.wait()
    for h in range(2):
        arrived(recv6.at[h], 12 + h, 15)
        mixed = jnp.sum(recv6[h].astype(F32), axis=0)
        send7[h] = (recv5[h, pl.ds(tp, 1)][0].astype(F32) + mixed).astype(BF16)
        to_group(send7.at[h], recv7.at[h], 14 + h)

    wd3t[...] = wd3[...].T
    newnrm_ref[...] = keep * nrm[...] + admit * key
    newstab_ref[...] = jnp.sum(jnp.where(eye, jnp.broadcast_to(new_stab, (16, 16)), 0.0), axis=0, keepdims=True)
    added = admit * key
    vh = value.astype(BF16)
    vl = (value - vh.astype(F32)).astype(BF16)
    vt = jnp.concatenate([vh.astype(F32), vl.astype(F32), vh.astype(F32)], axis=0).T.astype(BF16)
    row128 = lax.broadcasted_iota(jnp.int32, (16, 128), 0)
    kh = added.astype(BF16).astype(F32)
    kl = added - kh
    for b in range(16):
        khb = jnp.where(row128 == b, kh, 0.0)
        klb = jnp.where(row128 == b, kl, 0.0)
        outer = nn(vt, jnp.concatenate([khb, khb, klb], axis=0).astype(BF16))
        kb = jnp.sum(jnp.where(row128[:, :1] == b, keep, 0.0), axis=0, keepdims=True)
        memout[b] = kb * mem[b] + outer

    gain = gain_row(g3, kv)
    for h in range(2):
        from_group(recv7.at[h], arrived, 14 + h)
        gate_up(h, recv7[h].reshape(128, 256), gain, wg3, wu3, send8, recv8, 16 + h)
    for h in range(2):
        blk_t[h] = recv7[h].reshape(128, 256).T
    for h in range(2):
        second_sum(h, recv8, 16 + h, send8b, recv8b, 18 + h)
    for h in range(2):
        hidden(h, recv8b, 18 + h, recv9, 20 + h)

    for h in range(2):
        arrived(recv9.at[h], 20 + h, 15)
        send10[h] = nt(wd3t[...], recv9[h].reshape(128, 768)).astype(BF16).reshape(16, 16, 128)
        for t in tp_peers:
            send(send10.at[h, t], recv10.at[h, tp], 22 + h, kv, t)
        recv10[h, pl.ds(tp, 1)] = send10[h, pl.ds(tp, 1)]
    halves = []
    rows = pl.ds(pl.multiple_of(tp * 16, 16), 16)
    for h in range(2):
        arrived(recv10.at[h], 22 + h, 15)
        last = jnp.sum(recv10[h].astype(F32), axis=0)
        halves.append((blk_t[h, rows, :].astype(F32) + 0.5 * last).astype(BF16))
    res_ref[...] = nt(jnp.concatenate(halves, axis=1), order).astype(BF16)

    for h in range(2):
        sent(recv1.at[h], h, 15)
        sent(send2.at[h], 2 + h, 3)
        sent(send2b.at[h], 4 + h, 3)
        sent(recv3.at[h], 6 + h, 15)
        sent(send4.at[h], 8 + h, 15)
        from_group(recv5.at[h], sent, 10 + h)
        sent(send6.at[h], 12 + h, 15)
        from_group(recv7.at[h], sent, 14 + h)
        sent(send8.at[h], 16 + h, 3)
        sent(send8b.at[h], 18 + h, 3)
        sent(recv9.at[h], 20 + h, 15)
        sent(send10.at[h], 22 + h, 15)


def finish(res, mem, nrm, stab, res_out, mem_out, nrm_out, stab_out, sem):
    pairs = ((mem, mem_out), (res, res_out), (nrm, nrm_out), (stab, stab_out))
    copies = [pltpu.make_async_copy(s, d, sem.at[i]) for i, (s, d) in enumerate(pairs)]
    for c in copies:
        c.start()
    for c in copies:
        c.wait()


def layer(
    tokens, memory, normalizer, stabilizer, first_gain, first_gate, first_up, first_down, mixer_gain,
    query_weight, key_weight, value_weight, input_weight, forget_weight, forget_bias, output_weight,
    last_gain, last_gate, last_up, last_down,
):
    hbm = pl.BlockSpec(memory_space=pltpu.HBM)
    vmem = pl.BlockSpec(memory_space=pltpu.VMEM)
    b = lambda *s: pltpu.VMEM(s, BF16)
    f = lambda *s: pltpu.VMEM(s, F32)
    wide = lambda *s: b(2, 4, *s, WIDE)
    small = lambda: b(2, 16, 8, 256)
    scratch = [
        b(16, 256), f(16, 256, 128), b(16, 256, 128), f(16, 128), f(1, 16),
        f(32, 128), b(256, 768), b(256, 768), b(768, 256), f(32, 128),
        b(4096, 128), b(4096, 128), b(4096, 256), b(32, 4096), f(1, 1), b(256, 4096),
        f(32, 128), b(256, 768), b(256, 768), b(768, 256),
        b(2, 16, 16, 128), small(), wide(32), wide(32), wide(8), wide(8), b(2, 16, 8, 768),
        small(), small(), b(2, 8, 256), small(), b(16, 4096),
        small(), small(), b(2, 8, 256), small(), b(2, 256, 128),
        wide(32), wide(32), wide(8), wide(8), b(2, 16, 8, 768), b(256, 768),
        b(2, 16, 16, 128), b(2, 16, 16, 128),
        pltpu.SemaphoreType.DMA((20,)), pltpu.SemaphoreType.DMA((24,)), pltpu.SemaphoreType.DMA((24,)),
    ]
    shapes = (((16, 256), BF16), ((16, 256, 128), F32), ((16, 128), F32), ((1, 16), F32))
    parts = pl.pallas_call(
        kernel,
        out_shape=tuple(pltpu.VMEM(*s) for s in shapes),
        in_specs=[hbm] * 20,
        out_specs=(vmem,) * 4,
        scratch_shapes=scratch,
        compiler_params=pltpu.CompilerParams(
            collective_id=0, has_side_effects=True, vmem_limit_bytes=64_900_000
        ),
        name="layer",
    )(*(v for v in (
        tokens.T, memory.reshape(16, 256, 128), normalizer.reshape(16, 128), stabilizer.reshape(1, 16),
        first_gain.reshape(32, 128), first_gate, first_up, first_down, mixer_gain.reshape(32, 128),
        query_weight, key_weight, value_weight, input_weight.T, forget_weight.T,
        forget_bias.reshape(1, 1), output_weight, last_gain.reshape(32, 128), last_gate, last_up, last_down,
    )))
    res, new_mem, new_nrm, new_stab = pl.pallas_call(
        finish,
        out_shape=tuple(jax.ShapeDtypeStruct(*s) for s in shapes),
        in_specs=[vmem] * 4,
        out_specs=(hbm,) * 4,
        scratch_shapes=[pltpu.SemaphoreType.DMA((4,))],
        compiler_params=pltpu.CompilerParams(vmem_limit_bytes=1024 * 1024),
        name="finish",
    )(*(pltpu.with_memory_space_constraint(v, pltpu.VMEM) for v in parts))
    return res.T, new_mem.reshape(16, 1, 256, 128), new_nrm.reshape(16, 1, 128), new_stab.reshape(16, 1)


def solution(mesh):
    in_specs = (
        P(None, ("kv", "tp")), P("kv", "tp", None, None), P("kv", "tp", None), P("kv", "tp"), P(),
        P("kv", "tp"), P("kv", "tp"), P("tp", "kv"), P(), P(None, "tp"), P(None, "tp"), P(None, "tp"),
        P(), P(), P("tp"), P("tp", None), P(), P("kv", "tp"), P("kv", "tp"), P("tp", "kv"),
    )
    out_specs = (P(None, ("kv", "tp")), P("kv", "tp", None, None), P("kv", "tp", None), P("kv", "tp"))
    return jax.shard_map(layer, mesh=mesh, in_specs=in_specs, out_specs=out_specs, check_vma=False)
```

```python
import jax
import jax.numpy as jnp
from jax import lax
from jax.experimental import pallas as pl
from jax.experimental.pallas import tpu as pltpu
from jax.sharding import PartitionSpec as P

EPS = 1e-06
MESH = pl.DeviceIdType.MESH
F32 = jnp.float32
BF16 = jnp.bfloat16
KV_OFFSETS = (
    (2, 2), (1, 2), (2, 1), (3, 2), (2, 3), (1, 1), (3, 3), (1, 3),
    (3, 1), (0, 2), (2, 0), (0, 1), (1, 0), (0, 3), (3, 0),
)
TP_OFFSETS = (
    (4, 0), (4, 1), (3, 0), (5, 0), (3, 1), (5, 1), (2, 0), (6, 0),
    (2, 1), (6, 1), (1, 0), (7, 0), (1, 1), (7, 1), (0, 1),
)
WIDE = 1664


def nt(a, b):
    return lax.dot_general(a, b, (((1,), (1,)), ((), ())), preferred_element_type=F32)


def nn(a, b):
    return jnp.dot(a, b, preferred_element_type=F32)


def kernel(
    tok_hbm, mem_hbm, nrm_hbm, stab_hbm, g1_hbm, wg1_hbm, wu1_hbm, wd1_hbm, g2_hbm,
    wq_hbm, wk_hbm, wv_hbm, wi_hbm, wf_hbm, fb_hbm, wo_hbm, g3_hbm, wg3_hbm, wu3_hbm, wd3_hbm,
    res_ref, memout, newnrm_ref, newstab_ref,
    tok, mem, memb, nrm, stab, g1, wg1, wu1, wd1, g2, wq, wk, wv, wif, fb, wo, g3, wg3, wu3, wd3,
    recv1, blk, send2, recv2, send2b, recv2b, recv3, send4, recv4, send5, recv5, cell, send6, recv6,
    send7, recv7, blk_t, send8, recv8, send8b, recv8b, recv9, wd3t, send10, recv10,
    lsem, ssem, rsem,
):
    kv = lax.axis_index("kv")
    tp = lax.axis_index("tp")
    y, x = kv // 4, kv % 4
    z, core = tp // 2, tp % 2
    kv_peers = [lax.rem(y + dy, 4) * 4 + lax.rem(x + dx, 4) for dy, dx in KV_OFFSETS]
    tp_peers = [lax.rem(z + dz, 8) * 2 + lax.rem(core + dc, 2) for dz, dc in TP_OFFSETS]
    diag = kv == tp
    a_me = jnp.where(core == 0, x, y)
    b_me = jnp.where(core == 0, y, x)
    g_me = a_me * 4 + b_me
    a_peers = [lax.rem(a_me + d, 4) for d in (2, 1, 3)]
    b_peers = [lax.rem(b_me + d, 4) for d in (2, 1, 3)]

    def at(a, b):
        return jnp.where(core == 0, b * 4 + a, a * 4 + b)

    pairs = [
        (tok_hbm, tok), (wg1_hbm, wg1), (wu1_hbm, wu1), (g1_hbm, g1), (wd1_hbm, wd1),
        (wq_hbm, wq), (wk_hbm, wk), (wv_hbm, wv), (wi_hbm, wif.at[pl.ds(0, 16)]),
        (wf_hbm, wif.at[pl.ds(16, 16)]), (g2_hbm, g2), (mem_hbm, mem), (nrm_hbm, nrm),
        (stab_hbm, stab), (fb_hbm, fb), (wo_hbm, wo), (g3_hbm, g3), (wg3_hbm, wg3),
        (wu3_hbm, wu3), (wd3_hbm, wd3),
    ]
    loads = [pltpu.make_async_copy(s, d, lsem.at[i]) for i, (s, d) in enumerate(pairs)]
    for c in loads:
        c.start()
    (ld_tok, ld_wg1, ld_wu1, ld_g1, ld_wd1, ld_wq, ld_wk, ld_wv, ld_wi, ld_wf, ld_g2, ld_mem,
     ld_nrm, ld_stab, ld_fb, ld_wo, ld_g3, ld_wg3, ld_wu3, ld_wd3) = loads

    barrier = pltpu.get_barrier_semaphore()
    for k in kv_peers:
        pl.semaphore_signal(barrier, inc=1, device_id=(k, tp), device_id_type=MESH)
    for t in tp_peers:
        pl.semaphore_signal(barrier, inc=1, device_id=(kv, t), device_id_type=MESH)

    def send(src, dst, sem, k, t):
        pltpu.make_async_remote_copy(
            src_ref=src, dst_ref=dst, send_sem=ssem.at[sem], recv_sem=rsem.at[sem],
            device_id=(k, t), device_id_type=MESH,
        ).start()

    def arrived(buf, sem, count):
        part = buf.at[pl.ds(0, count)]
        pltpu.make_async_copy(part, part, rsem.at[sem]).wait()

    def sent(buf, sem, count):
        part = buf.at[pl.ds(0, count)]
        pltpu.make_async_copy(part, part, ssem.at[sem]).wait()

    def gain_row(g, c):
        return jnp.concatenate([g[pl.ds(2 * c, 1), :], g[pl.ds(2 * c + 1, 1), :]], axis=1)

    spot = lax.broadcasted_iota(jnp.int32, (256, 256), 1)
    seq = lax.broadcasted_iota(jnp.int32, (256, 256), 0)
    spot_row = ((spot % 128) // 8) * 16 + (spot // 128) * 8 + spot % 8
    order = jnp.where(seq == spot_row, 1.0, 0.0).astype(BF16)
    ld_tok.wait()
    ordered = nn(tok[...], order).astype(BF16)
    for h in range(2):
        recv1[h, pl.ds(tp, 1)] = ordered[:, h * 128 : h * 128 + 128][None]
    pl.semaphore_wait(barrier, 30)

    for h in range(2):
        for t in tp_peers:
            send(recv1.at[h, tp], recv1.at[h, tp], h, kv, t)

    def gate_up(h, block, gain, wg, wu, out, into, sem):
        vals = block.astype(F32)
        scaled = (vals * gain).astype(BF16)
        sq = jnp.sum(vals * vals, axis=1, keepdims=True)
        out[h, :, :, pl.ds(1536, 128)] = jnp.broadcast_to(sq, (128, 128)).astype(BF16).reshape(4, 32, 128)
        for n in range(3):
            cols = pl.ds(n * 256, 256)
            out[h, :, :, cols] = nn(scaled, wg[:, cols]).astype(BF16).reshape(4, 32, 256)
            out[h, :, :, pl.ds(768 + n * 256, 256)] = nn(scaled, wu[:, cols]).astype(BF16).reshape(4, 32, 256)
        for a in a_peers:
            send(out.at[h, a], into.at[h, a_me], sem, at(a, b_me), tp)
        into[h, pl.ds(a_me, 1)] = out[h, pl.ds(a_me, 1)]

    def second_sum(h, into, sem, out, next_into, next_sem):
        arrived(into.at[h], sem, 3)
        for n in range(0, WIDE, 128):
            cols = pl.ds(n, 128)
            total = jnp.sum(into[h, :, :, cols].astype(F32), axis=0)
            out[h, :, :, cols] = total.reshape(4, 8, 128).astype(BF16)
        for b in b_peers:
            send(out.at[h, b], next_into.at[h, b_me], next_sem, at(a_me, b), tp)
        next_into[h, pl.ds(b_me, 1)] = out[h, pl.ds(b_me, 1)]

    def hidden(h, into, sem, gathered, next_sem):
        arrived(into.at[h], sem, 3)
        total = jnp.sum(into[h].astype(F32), axis=0)
        scale = lax.rsqrt(total[:, 1536:1537] / 4096 + EPS)
        gate = scale * total[:, :768]
        up = scale * total[:, 768:1536]
        gathered[h, pl.ds(g_me, 1)] = (gate / (1.0 + jnp.exp(-gate)) * up).astype(BF16)[None]
        for k in kv_peers:
            send(gathered.at[h, g_me], gathered.at[h, g_me], next_sem, k, tp)

    def to_group(buf, into, sem):
        for t in tp_peers:
            send(buf, into.at[kv], sem, tp, t)

        @pl.when(jnp.logical_not(diag))
        def _():
            send(buf, into.at[kv], sem, tp, tp)

        @pl.when(diag)
        def _():
            into[pl.ds(kv, 1)] = buf[...][None]

    def from_group(buf, wait, sem):
        @pl.when(diag)
        def _():
            wait(buf, sem, 15)

        @pl.when(jnp.logical_not(diag))
        def _():
            wait(buf, sem, 16)

    gain = None
    for h in range(2):
        arrived(recv1.at[h], h, 15)
        block = recv1[h].reshape(256, 128).T
        blk[h] = block.reshape(16, 8, 256)
        if h == 0:
            ld_wg1.wait()
            ld_wu1.wait()
            ld_g1.wait()
            gain = gain_row(g1, kv)
        gate_up(h, block, gain, wg1, wu1, send2, recv2, 2 + h)
    for h in range(2):
        second_sum(h, recv2, 2 + h, send2b, recv2b, 4 + h)
    for h in range(2):
        hidden(h, recv2b, 4 + h, recv3, 6 + h)

    ld_wd1.wait()
    for h in range(2):
        arrived(recv3.at[h], 6 + h, 15)
        send4[h] = nn(recv3[h].reshape(128, 768), wd1[...]).astype(BF16).reshape(16, 8, 256)
        for t in tp_peers:
            send(send4.at[h, t], recv4.at[h, tp], 8 + h, kv, t)
        recv4[h, pl.ds(tp, 1)] = send4[h, pl.ds(tp, 1)]
    for c in (ld_wq, ld_wk, ld_wv, ld_wi, ld_wf, ld_g2, ld_nrm, ld_stab, ld_fb, ld_mem, ld_wo):
        c.wait()
    memb[...] = mem[...].astype(BF16)

    for h in range(2):
        arrived(recv4.at[h], 8 + h, 15)
        first = jnp.sum(recv4[h].astype(F32), axis=0)
        send5[h] = (blk[h, pl.ds(tp, 1)][0].astype(F32) + 0.5 * first).astype(BF16)
        to_group(send5.at[h], recv5.at[h], 10 + h)
    for h in range(2):
        from_group(recv5.at[h], arrived, 10 + h)

    sq = jnp.zeros((16, 256), F32)
    for c in range(16):
        v = jnp.concatenate([recv5[0, c].astype(F32), recv5[1, c].astype(F32)], axis=0)
        sq = sq + v * v
        cell[:, pl.ds(c * 256, 256)] = (v * gain_row(g2, c)).astype(BF16)
    scale = lax.rsqrt(jnp.sum(sq, axis=1, keepdims=True) / 4096 + EPS)
    query = scale * nn(cell[...], wq[...]) * 128 ** (-0.5)
    key = scale * nn(cell[...], wk[...])
    value = scale * nn(cell[...], wv[...])
    gates = nt(cell[...], wif[...])
    lane32 = lax.broadcasted_iota(jnp.int32, (16, 32), 1)
    input_pre = scale * jnp.sum(jnp.where(lane32 == tp, gates, 0.0), axis=1, keepdims=True)
    pre = scale * jnp.sum(jnp.where(lane32 == tp + 16, gates, 0.0), axis=1, keepdims=True) + fb[...]
    log_forget = jnp.minimum(pre, 0.0) - jnp.log1p(jnp.exp(-jnp.abs(pre)))
    eye = lax.broadcasted_iota(jnp.int32, (16, 16), 0) == lax.broadcasted_iota(jnp.int32, (16, 16), 1)
    old_stab = jnp.sum(jnp.where(eye, jnp.broadcast_to(stab[...], (16, 16)), 0.0), axis=1, keepdims=True)
    carried = log_forget + old_stab
    new_stab = jnp.maximum(carried, input_pre)
    keep = jnp.exp(carried - new_stab)
    admit = jnp.exp(input_pre - new_stab)
    match = jnp.sum(query * key, axis=1, keepdims=True)
    denom = keep * jnp.sum(nrm[...] * query, axis=1, keepdims=True) + admit * match
    qb = query.astype(BF16)
    row256 = lax.broadcasted_iota(jnp.int32, (16, 256), 0)
    recalled = jnp.zeros((16, 256), F32)
    for b in range(16):
        recalled = jnp.where(row256 == b, nt(qb, memb[b]), recalled)
    numer = keep * recalled + (admit * match) * value
    cell_out = (numer / jnp.maximum(jnp.abs(denom), 1.0)).astype(BF16)

    for c in range(16):
        send6[:, c] = nn(cell_out, wo[:, pl.ds(c * 256, 256)]).astype(BF16).reshape(2, 8, 256)
    for h in range(2):
        for t in tp_peers:
            send(send6.at[h, t], recv6.at[h, tp], 12 + h, kv, t)
        recv6[h, pl.ds(tp, 1)] = send6[h, pl.ds(tp, 1)]

    for c in (ld_wg3, ld_wu3, ld_g3, ld_wd3):
        c.wait()
    for h in range(2):
        arrived(recv6.at[h], 12 + h, 15)
        mixed = jnp.sum(recv6[h].astype(F32), axis=0)
        send7[h] = (recv5[h, pl.ds(tp, 1)][0].astype(F32) + mixed).astype(BF16)
        to_group(send7.at[h], recv7.at[h], 14 + h)

    wd3t[...] = wd3[...].T
    newnrm_ref[...] = keep * nrm[...] + admit * key
    newstab_ref[...] = jnp.sum(jnp.where(eye, jnp.broadcast_to(new_stab, (16, 16)), 0.0), axis=0, keepdims=True)
    added = admit * key
    vh = value.astype(BF16)
    vl = (value - vh.astype(F32)).astype(BF16)
    vt = jnp.concatenate([vh.astype(F32), vl.astype(F32), vh.astype(F32)], axis=0).T.astype(BF16)
    row128 = lax.broadcasted_iota(jnp.int32, (16, 128), 0)
    kh = added.astype(BF16).astype(F32)
    kl = added - kh
    for b in range(16):
        khb = jnp.where(row128 == b, kh, 0.0)
        klb = jnp.where(row128 == b, kl, 0.0)
        outer = nn(vt, jnp.concatenate([khb, khb, klb], axis=0).astype(BF16))
        kb = jnp.sum(jnp.where(row128[:, :1] == b, keep, 0.0), axis=0, keepdims=True)
        memout[b] = kb * mem[b] + outer

    gain = gain_row(g3, kv)
    for h in range(2):
        from_group(recv7.at[h], arrived, 14 + h)
        gate_up(h, recv7[h].reshape(128, 256), gain, wg3, wu3, send8, recv8, 16 + h)
    for h in range(2):
        blk_t[h] = recv7[h].reshape(128, 256).T
    for h in range(2):
        second_sum(h, recv8, 16 + h, send8b, recv8b, 18 + h)
    for h in range(2):
        hidden(h, recv8b, 18 + h, recv9, 20 + h)

    for h in range(2):
        arrived(recv9.at[h], 20 + h, 15)
        send10[h] = nt(wd3t[...], recv9[h].reshape(128, 768)).astype(BF16).reshape(16, 16, 128)
        for t in tp_peers:
            send(send10.at[h, t], recv10.at[h, tp], 22 + h, kv, t)
        recv10[h, pl.ds(tp, 1)] = send10[h, pl.ds(tp, 1)]
    halves = []
    rows = pl.ds(pl.multiple_of(tp * 16, 16), 16)
    for h in range(2):
        arrived(recv10.at[h], 22 + h, 15)
        last = jnp.sum(recv10[h].astype(F32), axis=0)
        halves.append((blk_t[h, rows, :].astype(F32) + 0.5 * last).astype(BF16))
    res_ref[...] = nt(jnp.concatenate(halves, axis=1), order).astype(BF16)

    for h in range(2):
        sent(recv1.at[h], h, 15)
        sent(send2.at[h], 2 + h, 3)
        sent(send2b.at[h], 4 + h, 3)
        sent(recv3.at[h], 6 + h, 15)
        sent(send4.at[h], 8 + h, 15)
        from_group(recv5.at[h], sent, 10 + h)
        sent(send6.at[h], 12 + h, 15)
        from_group(recv7.at[h], sent, 14 + h)
        sent(send8.at[h], 16 + h, 3)
        sent(send8b.at[h], 18 + h, 3)
        sent(recv9.at[h], 20 + h, 15)
        sent(send10.at[h], 22 + h, 15)


def finish(res, mem, nrm, stab, res_out, mem_out, nrm_out, stab_out, sem):
    pairs = ((mem, mem_out), (res, res_out), (nrm, nrm_out), (stab, stab_out))
    copies = [pltpu.make_async_copy(s, d, sem.at[i]) for i, (s, d) in enumerate(pairs)]
    for c in copies:
        c.start()
    for c in copies:
        c.wait()


def layer(
    tokens, memory, normalizer, stabilizer, first_gain, first_gate, first_up, first_down, mixer_gain,
    query_weight, key_weight, value_weight, input_weight, forget_weight, forget_bias, output_weight,
    last_gain, last_gate, last_up, last_down,
):
    hbm = pl.BlockSpec(memory_space=pltpu.HBM)
    vmem = pl.BlockSpec(memory_space=pltpu.VMEM)
    b = lambda *s: pltpu.VMEM(s, BF16)
    f = lambda *s: pltpu.VMEM(s, F32)
    wide = lambda *s: b(2, 4, *s, WIDE)
    small = lambda: b(2, 16, 8, 256)
    scratch = [
        b(16, 256), f(16, 256, 128), b(16, 256, 128), f(16, 128), f(1, 16),
        f(32, 128), b(256, 768), b(256, 768), b(768, 256), f(32, 128),
        b(4096, 128), b(4096, 128), b(4096, 256), b(32, 4096), f(1, 1), b(256, 4096),
        f(32, 128), b(256, 768), b(256, 768), b(768, 256),
        b(2, 16, 16, 128), small(), wide(32), wide(32), wide(8), wide(8), b(2, 16, 8, 768),
        small(), small(), b(2, 8, 256), small(), b(16, 4096),
        small(), small(), b(2, 8, 256), small(), b(2, 256, 128),
        wide(32), wide(32), wide(8), wide(8), b(2, 16, 8, 768), b(256, 768),
        b(2, 16, 16, 128), b(2, 16, 16, 128),
        pltpu.SemaphoreType.DMA((20,)), pltpu.SemaphoreType.DMA((24,)), pltpu.SemaphoreType.DMA((24,)),
    ]
    shapes = (((16, 256), BF16), ((16, 256, 128), F32), ((16, 128), F32), ((1, 16), F32))
    parts = pl.pallas_call(
        kernel,
        out_shape=tuple(pltpu.VMEM(*s) for s in shapes),
        in_specs=[hbm] * 20,
        out_specs=(vmem,) * 4,
        scratch_shapes=scratch,
        compiler_params=pltpu.CompilerParams(
            collective_id=0, has_side_effects=True, vmem_limit_bytes=64_900_000
        ),
        name="layer",
    )(*(v for v in (
        tokens.T, memory.reshape(16, 256, 128), normalizer.reshape(16, 128), stabilizer.reshape(1, 16),
        first_gain.reshape(32, 128), first_gate, first_up, first_down, mixer_gain.reshape(32, 128),
        query_weight, key_weight, value_weight, input_weight.T, forget_weight.T,
        forget_bias.reshape(1, 1), output_weight, last_gain.reshape(32, 128), last_gate, last_up, last_down,
    )))
    res, new_mem, new_nrm, new_stab = pl.pallas_call(
        finish,
        out_shape=tuple(jax.ShapeDtypeStruct(*s) for s in shapes),
        in_specs=[vmem] * 4,
        out_specs=(hbm,) * 4,
        scratch_shapes=[pltpu.SemaphoreType.DMA((4,))],
        compiler_params=pltpu.CompilerParams(vmem_limit_bytes=1024 * 1024),
        name="finish",
    )(*(pltpu.with_memory_space_constraint(v, pltpu.VMEM) for v in parts))
    return res.T, new_mem.reshape(16, 1, 256, 128), new_nrm.reshape(16, 1, 128), new_stab.reshape(16, 1)


def solution(mesh):
    in_specs = (
        P(None, ("kv", "tp")), P("kv", "tp", None, None), P("kv", "tp", None), P("kv", "tp"), P(),
        P("kv", "tp"), P("kv", "tp"), P("tp", "kv"), P(), P(None, "tp"), P(None, "tp"), P(None, "tp"),
        P(), P(), P("tp"), P("tp", None), P(), P("kv", "tp"), P("kv", "tp"), P("tp", "kv"),
    )
    out_specs = (P(None, ("kv", "tp")), P("kv", "tp", None, None), P("kv", "tp", None), P("kv", "tp"))
    return jax.shard_map(layer, mesh=mesh, in_specs=in_specs, out_specs=out_specs, check_vma=False)
```

```python
import jax
import jax.numpy as jnp
from jax import lax
from jax.experimental import pallas as pl
from jax.experimental.pallas import tpu as pltpu
from jax.sharding import PartitionSpec as P

EPS = 1e-06
MESH = pl.DeviceIdType.MESH
F32 = jnp.float32
BF16 = jnp.bfloat16
KV_OFFSETS = (
    (2, 2), (1, 2), (2, 1), (3, 2), (2, 3), (1, 1), (3, 3), (1, 3),
    (3, 1), (0, 2), (2, 0), (0, 1), (1, 0), (0, 3), (3, 0),
)
TP_OFFSETS = (
    (4, 0), (4, 1), (3, 0), (5, 0), (3, 1), (5, 1), (2, 0), (6, 0),
    (2, 1), (6, 1), (1, 0), (7, 0), (1, 1), (7, 1), (0, 1),
)
WIDE = 1664


def nt(a, b):
    return lax.dot_general(a, b, (((1,), (1,)), ((), ())), preferred_element_type=F32)


def nn(a, b):
    return jnp.dot(a, b, preferred_element_type=F32)


def kernel(
    tok_hbm, mem_hbm, nrm_hbm, stab_hbm, g1_hbm, wg1_hbm, wu1_hbm, wd1_hbm, g2_hbm,
    wq_hbm, wk_hbm, wv_hbm, wi_hbm, wf_hbm, fb_hbm, wo_hbm, g3_hbm, wg3_hbm, wu3_hbm, wd3_hbm,
    res_ref, memout, newnrm_ref, newstab_ref,
    tok, mem, memb, nrm, stab, g1, wg1, wu1, wd1, g2, wq, wk, wv, wif, fb, wo, g3, wg3, wu3, wd3,
    recv1, blk, send2, recv2, send2b, recv2b, recv3, send4, recv4, send5, recv5, cell, send6, recv6,
    send7, recv7, blk_t, send8, recv8, send8b, recv8b, recv9, wd3t, send10, recv10,
    lsem, ssem, rsem,
):
    kv = lax.axis_index("kv")
    tp = lax.axis_index("tp")
    y, x = kv // 4, kv % 4
    z, core = tp // 2, tp % 2
    kv_peers = [lax.rem(y + dy, 4) * 4 + lax.rem(x + dx, 4) for dy, dx in KV_OFFSETS]
    tp_peers = [lax.rem(z + dz, 8) * 2 + lax.rem(core + dc, 2) for dz, dc in TP_OFFSETS]
    diag = kv == tp
    a_me = jnp.where(core == 1, x, y)
    b_me = jnp.where(core == 1, y, x)
    g_me = a_me * 4 + b_me
    a_peers = [lax.rem(a_me + d, 4) for d in (2, 3, 1)]
    b_peers = [lax.rem(b_me + d, 4) for d in (2, 3, 1)]

    def at(a, b):
        return jnp.where(core == 1, b * 4 + a, a * 4 + b)

    pairs = [
        (tok_hbm, tok), (wg1_hbm, wg1), (wu1_hbm, wu1), (g1_hbm, g1), (wd1_hbm, wd1),
        (wq_hbm, wq), (wk_hbm, wk), (wv_hbm, wv), (wi_hbm, wif.at[pl.ds(0, 16)]),
        (wf_hbm, wif.at[pl.ds(16, 16)]), (g2_hbm, g2), (mem_hbm, mem), (nrm_hbm, nrm),
        (stab_hbm, stab), (fb_hbm, fb), (wo_hbm, wo), (g3_hbm, g3), (wg3_hbm, wg3),
        (wu3_hbm, wu3), (wd3_hbm, wd3),
    ]
    loads = [pltpu.make_async_copy(s, d, lsem.at[i]) for i, (s, d) in enumerate(pairs)]
    for c in loads:
        c.start()
    (ld_tok, ld_wg1, ld_wu1, ld_g1, ld_wd1, ld_wq, ld_wk, ld_wv, ld_wi, ld_wf, ld_g2, ld_mem,
     ld_nrm, ld_stab, ld_fb, ld_wo, ld_g3, ld_wg3, ld_wu3, ld_wd3) = loads

    barrier = pltpu.get_barrier_semaphore()
    for k in kv_peers:
        pl.semaphore_signal(barrier, inc=1, device_id=(k, tp), device_id_type=MESH)
    for t in tp_peers:
        pl.semaphore_signal(barrier, inc=1, device_id=(kv, t), device_id_type=MESH)

    def send(src, dst, sem, k, t):
        pltpu.make_async_remote_copy(
            src_ref=src, dst_ref=dst, send_sem=ssem.at[sem], recv_sem=rsem.at[sem],
            device_id=(k, t), device_id_type=MESH,
        ).start()

    def arrived(buf, sem, count):
        part = buf.at[pl.ds(0, count)]
        pltpu.make_async_copy(part, part, rsem.at[sem]).wait()

    def sent(buf, sem, count):
        part = buf.at[pl.ds(0, count)]
        pltpu.make_async_copy(part, part, ssem.at[sem]).wait()

    def gain_row(g, c):
        return jnp.concatenate([g[pl.ds(2 * c, 1), :], g[pl.ds(2 * c + 1, 1), :]], axis=1)

    spot = lax.broadcasted_iota(jnp.int32, (256, 256), 1)
    seq = lax.broadcasted_iota(jnp.int32, (256, 256), 0)
    spot_row = ((spot % 128) // 8) * 16 + (spot // 128) * 8 + spot % 8
    order = jnp.where(seq == spot_row, 1.0, 0.0).astype(BF16)
    ld_tok.wait()
    ordered = nn(tok[...], order).astype(BF16)
    for h in range(2):
        recv1[h, pl.ds(tp, 1)] = ordered[:, h * 128 : h * 128 + 128][None]
    pl.semaphore_wait(barrier, 30)

    for h in range(2):
        for t in tp_peers:
            send(recv1.at[h, tp], recv1.at[h, tp], h, kv, t)

    def gate_up(h, block, gain, wg, wu, out, into, sem):
        vals = block.astype(F32)
        scaled = (vals * gain).astype(BF16)
        sq = jnp.sum(vals * vals, axis=1, keepdims=True)
        out[h, :, :, pl.ds(1536, 128)] = jnp.broadcast_to(sq, (128, 128)).astype(BF16).reshape(4, 32, 128)
        for n in range(3):
            cols = pl.ds(n * 256, 256)
            out[h, :, :, cols] = nn(scaled, wg[:, cols]).astype(BF16).reshape(4, 32, 256)
            out[h, :, :, pl.ds(768 + n * 256, 256)] = nn(scaled, wu[:, cols]).astype(BF16).reshape(4, 32, 256)
        for a in a_peers:
            send(out.at[h, a], into.at[h, a_me], sem, at(a, b_me), tp)
        into[h, pl.ds(a_me, 1)] = out[h, pl.ds(a_me, 1)]

    def second_sum(h, into, sem, out, next_into, next_sem):
        arrived(into.at[h], sem, 3)
        for n in range(0, WIDE, 128):
            cols = pl.ds(n, 128)
            total = jnp.sum(into[h, :, :, cols].astype(F32), axis=0)
            out[h, :, :, cols] = total.reshape(4, 8, 128).astype(BF16)
        for b in b_peers:
            send(out.at[h, b], next_into.at[h, b_me], next_sem, at(a_me, b), tp)
        next_into[h, pl.ds(b_me, 1)] = out[h, pl.ds(b_me, 1)]

    def hidden(h, into, sem, gathered, next_sem):
        arrived(into.at[h], sem, 3)
        total = jnp.sum(into[h].astype(F32), axis=0)
        scale = lax.rsqrt(total[:, 1536:1537] / 4096 + EPS)
        gate = scale * total[:, :768]
        up = scale * total[:, 768:1536]
        gathered[h, pl.ds(g_me, 1)] = (gate / (1.0 + jnp.exp(-gate)) * up).astype(BF16)[None]
        for k in kv_peers:
            send(gathered.at[h, g_me], gathered.at[h, g_me], next_sem, k, tp)

    def to_group(buf, into, sem):
        for t in tp_peers:
            send(buf, into.at[kv], sem, tp, t)

        @pl.when(jnp.logical_not(diag))
        def _():
            send(buf, into.at[kv], sem, tp, tp)

        @pl.when(diag)
        def _():
            into[pl.ds(kv, 1)] = buf[...][None]

    def from_group(buf, wait, sem):
        @pl.when(diag)
        def _():
            wait(buf, sem, 15)

        @pl.when(jnp.logical_not(diag))
        def _():
            wait(buf, sem, 16)

    gain = None
    for h in range(2):
        arrived(recv1.at[h], h, 15)
        block = recv1[h].reshape(256, 128).T
        blk[h] = block.reshape(16, 8, 256)
        if h == 0:
            ld_wg1.wait()
            ld_wu1.wait()
            ld_g1.wait()
            gain = gain_row(g1, kv)
        gate_up(h, block, gain, wg1, wu1, send2, recv2, 2 + h)
    for h in range(2):
        second_sum(h, recv2, 2 + h, send2b, recv2b, 4 + h)
    for h in range(2):
        hidden(h, recv2b, 4 + h, recv3, 6 + h)

    ld_wd1.wait()
    for h in range(2):
        arrived(recv3.at[h], 6 + h, 15)
        send4[h] = nn(recv3[h].reshape(128, 768), wd1[...]).astype(BF16).reshape(16, 8, 256)
        for t in tp_peers:
            send(send4.at[h, t], recv4.at[h, tp], 8 + h, kv, t)
        recv4[h, pl.ds(tp, 1)] = send4[h, pl.ds(tp, 1)]
    for c in (ld_wq, ld_wk, ld_wv, ld_wi, ld_wf, ld_g2, ld_nrm, ld_stab, ld_fb, ld_mem, ld_wo):
        c.wait()
    memb[...] = mem[...].astype(BF16)

    for h in range(2):
        arrived(recv4.at[h], 8 + h, 15)
        first = jnp.sum(recv4[h].astype(F32), axis=0)
        send5[h] = (blk[h, pl.ds(tp, 1)][0].astype(F32) + 0.5 * first).astype(BF16)
        to_group(send5.at[h], recv5.at[h], 10 + h)
    for h in range(2):
        from_group(recv5.at[h], arrived, 10 + h)

    sq = jnp.zeros((16, 256), F32)
    for c in range(16):
        v = jnp.concatenate([recv5[0, c].astype(F32), recv5[1, c].astype(F32)], axis=0)
        sq = sq + v * v
        cell[:, pl.ds(c * 256, 256)] = (v * gain_row(g2, c)).astype(BF16)
    scale = lax.rsqrt(jnp.sum(sq, axis=1, keepdims=True) / 4096 + EPS)
    query = scale * nn(cell[...], wq[...]) * 128 ** (-0.5)
    key = scale * nn(cell[...], wk[...])
    value = scale * nn(cell[...], wv[...])
    gates = nt(cell[...], wif[...])
    lane32 = lax.broadcasted_iota(jnp.int32, (16, 32), 1)
    input_pre = scale * jnp.sum(jnp.where(lane32 == tp, gates, 0.0), axis=1, keepdims=True)
    pre = scale * jnp.sum(jnp.where(lane32 == tp + 16, gates, 0.0), axis=1, keepdims=True) + fb[...]
    log_forget = jnp.minimum(pre, 0.0) - jnp.log1p(jnp.exp(-jnp.abs(pre)))
    eye = lax.broadcasted_iota(jnp.int32, (16, 16), 0) == lax.broadcasted_iota(jnp.int32, (16, 16), 1)
    old_stab = jnp.sum(jnp.where(eye, jnp.broadcast_to(stab[...], (16, 16)), 0.0), axis=1, keepdims=True)
    carried = log_forget + old_stab
    new_stab = jnp.maximum(carried, input_pre)
    keep = jnp.exp(carried - new_stab)
    admit = jnp.exp(input_pre - new_stab)
    match = jnp.sum(query * key, axis=1, keepdims=True)
    denom = keep * jnp.sum(nrm[...] * query, axis=1, keepdims=True) + admit * match
    qb = query.astype(BF16)
    row256 = lax.broadcasted_iota(jnp.int32, (16, 256), 0)
    recalled = jnp.zeros((16, 256), F32)
    for b in range(16):
        recalled = jnp.where(row256 == b, nt(qb, memb[b]), recalled)
    numer = keep * recalled + (admit * match) * value
    cell_out = (numer / jnp.maximum(jnp.abs(denom), 1.0)).astype(BF16)

    for c in range(16):
        send6[:, c] = nn(cell_out, wo[:, pl.ds(c * 256, 256)]).astype(BF16).reshape(2, 8, 256)
    for h in range(2):
        for t in tp_peers:
            send(send6.at[h, t], recv6.at[h, tp], 12 + h, kv, t)
        recv6[h, pl.ds(tp, 1)] = send6[h, pl.ds(tp, 1)]

    for c in (ld_wg3, ld_wu3, ld_g3, ld_wd3):
        c.wait()
    for h in range(2):
        arrived(recv6.at[h], 12 + h, 15)
        mixed = jnp.sum(recv6[h].astype(F32), axis=0)
        send7[h] = (recv5[h, pl.ds(tp, 1)][0].astype(F32) + mixed).astype(BF16)
        to_group(send7.at[h], recv7.at[h], 14 + h)

    wd3t[...] = wd3[...].T
    newnrm_ref[...] = keep * nrm[...] + admit * key
    newstab_ref[...] = jnp.sum(jnp.where(eye, jnp.broadcast_to(new_stab, (16, 16)), 0.0), axis=0, keepdims=True)
    added = admit * key
    vh = value.astype(BF16)
    vl = (value - vh.astype(F32)).astype(BF16)
    vt = jnp.concatenate([vh.astype(F32), vl.astype(F32), vh.astype(F32)], axis=0).T.astype(BF16)
    row128 = lax.broadcasted_iota(jnp.int32, (16, 128), 0)
    kh = added.astype(BF16).astype(F32)
    kl = added - kh
    for b in range(16):
        khb = jnp.where(row128 == b, kh, 0.0)
        klb = jnp.where(row128 == b, kl, 0.0)
        outer = nn(vt, jnp.concatenate([khb, khb, klb], axis=0).astype(BF16))
        kb = jnp.sum(jnp.where(row128[:, :1] == b, keep, 0.0), axis=0, keepdims=True)
        memout[b] = kb * mem[b] + outer

    gain = gain_row(g3, kv)
    for h in range(2):
        from_group(recv7.at[h], arrived, 14 + h)
        gate_up(h, recv7[h].reshape(128, 256), gain, wg3, wu3, send8, recv8, 16 + h)
    for h in range(2):
        blk_t[h] = recv7[h].reshape(128, 256).T
    for h in range(2):
        second_sum(h, recv8, 16 + h, send8b, recv8b, 18 + h)
    for h in range(2):
        hidden(h, recv8b, 18 + h, recv9, 20 + h)

    for h in range(2):
        arrived(recv9.at[h], 20 + h, 15)
        send10[h] = nt(wd3t[...], recv9[h].reshape(128, 768)).astype(BF16).reshape(16, 16, 128)
        for t in tp_peers:
            send(send10.at[h, t], recv10.at[h, tp], 22 + h, kv, t)
        recv10[h, pl.ds(tp, 1)] = send10[h, pl.ds(tp, 1)]
    halves = []
    rows = pl.ds(pl.multiple_of(tp * 16, 16), 16)
    for h in range(2):
        arrived(recv10.at[h], 22 + h, 15)
        last = jnp.sum(recv10[h].astype(F32), axis=0)
        halves.append((blk_t[h, rows, :].astype(F32) + 0.5 * last).astype(BF16))
    res_ref[...] = nt(jnp.concatenate(halves, axis=1), order).astype(BF16)

    for h in range(2):
        sent(recv1.at[h], h, 15)
        sent(send2.at[h], 2 + h, 3)
        sent(send2b.at[h], 4 + h, 3)
        sent(recv3.at[h], 6 + h, 15)
        sent(send4.at[h], 8 + h, 15)
        from_group(recv5.at[h], sent, 10 + h)
        sent(send6.at[h], 12 + h, 15)
        from_group(recv7.at[h], sent, 14 + h)
        sent(send8.at[h], 16 + h, 3)
        sent(send8b.at[h], 18 + h, 3)
        sent(recv9.at[h], 20 + h, 15)
        sent(send10.at[h], 22 + h, 15)


def finish(res, mem, nrm, stab, res_out, mem_out, nrm_out, stab_out, sem):
    pairs = ((mem, mem_out), (res, res_out), (nrm, nrm_out), (stab, stab_out))
    copies = [pltpu.make_async_copy(s, d, sem.at[i]) for i, (s, d) in enumerate(pairs)]
    for c in copies:
        c.start()
    for c in copies:
        c.wait()


def layer(
    tokens, memory, normalizer, stabilizer, first_gain, first_gate, first_up, first_down, mixer_gain,
    query_weight, key_weight, value_weight, input_weight, forget_weight, forget_bias, output_weight,
    last_gain, last_gate, last_up, last_down,
):
    hbm = pl.BlockSpec(memory_space=pltpu.HBM)
    vmem = pl.BlockSpec(memory_space=pltpu.VMEM)
    b = lambda *s: pltpu.VMEM(s, BF16)
    f = lambda *s: pltpu.VMEM(s, F32)
    wide = lambda *s: b(2, 4, *s, WIDE)
    small = lambda: b(2, 16, 8, 256)
    scratch = [
        b(16, 256), f(16, 256, 128), b(16, 256, 128), f(16, 128), f(1, 16),
        f(32, 128), b(256, 768), b(256, 768), b(768, 256), f(32, 128),
        b(4096, 128), b(4096, 128), b(4096, 256), b(32, 4096), f(1, 1), b(256, 4096),
        f(32, 128), b(256, 768), b(256, 768), b(768, 256),
        b(2, 16, 16, 128), small(), wide(32), wide(32), wide(8), wide(8), b(2, 16, 8, 768),
        small(), small(), b(2, 8, 256), small(), b(16, 4096),
        small(), small(), b(2, 8, 256), small(), b(2, 256, 128),
        wide(32), wide(32), wide(8), wide(8), b(2, 16, 8, 768), b(256, 768),
        b(2, 16, 16, 128), b(2, 16, 16, 128),
        pltpu.SemaphoreType.DMA((20,)), pltpu.SemaphoreType.DMA((24,)), pltpu.SemaphoreType.DMA((24,)),
    ]
    shapes = (((16, 256), BF16), ((16, 256, 128), F32), ((16, 128), F32), ((1, 16), F32))
    parts = pl.pallas_call(
        kernel,
        out_shape=tuple(pltpu.VMEM(*s) for s in shapes),
        in_specs=[hbm] * 20,
        out_specs=(vmem,) * 4,
        scratch_shapes=scratch,
        compiler_params=pltpu.CompilerParams(
            collective_id=0, has_side_effects=True, vmem_limit_bytes=64_900_000
        ),
        name="layer",
    )(*(v for v in (
        tokens.T, memory.reshape(16, 256, 128), normalizer.reshape(16, 128), stabilizer.reshape(1, 16),
        first_gain.reshape(32, 128), first_gate, first_up, first_down, mixer_gain.reshape(32, 128),
        query_weight, key_weight, value_weight, input_weight.T, forget_weight.T,
        forget_bias.reshape(1, 1), output_weight, last_gain.reshape(32, 128), last_gate, last_up, last_down,
    )))
    res, new_mem, new_nrm, new_stab = pl.pallas_call(
        finish,
        out_shape=tuple(jax.ShapeDtypeStruct(*s) for s in shapes),
        in_specs=[vmem] * 4,
        out_specs=(hbm,) * 4,
        scratch_shapes=[pltpu.SemaphoreType.DMA((4,))],
        compiler_params=pltpu.CompilerParams(vmem_limit_bytes=1024 * 1024),
        name="finish",
    )(*(pltpu.with_memory_space_constraint(v, pltpu.VMEM) for v in parts))
    return res.T, new_mem.reshape(16, 1, 256, 128), new_nrm.reshape(16, 1, 128), new_stab.reshape(16, 1)


def solution(mesh):
    in_specs = (
        P(None, ("kv", "tp")), P("kv", "tp", None, None), P("kv", "tp", None), P("kv", "tp"), P(),
        P("kv", "tp"), P("kv", "tp"), P("tp", "kv"), P(), P(None, "tp"), P(None, "tp"), P(None, "tp"),
        P(), P(), P("tp"), P("tp", None), P(), P("kv", "tp"), P("kv", "tp"), P("tp", "kv"),
    )
    out_specs = (P(None, ("kv", "tp")), P("kv", "tp", None, None), P("kv", "tp", None), P("kv", "tp"))
    return jax.shard_map(layer, mesh=mesh, in_specs=in_specs, out_specs=out_specs, check_vma=False)
```

```python
import jax
import jax.numpy as jnp
from jax import lax
from jax.experimental import pallas as pl
from jax.experimental.pallas import tpu as pltpu
from jax.sharding import PartitionSpec as P

EPS = 1e-06
MESH = pl.DeviceIdType.MESH
F32 = jnp.float32
BF16 = jnp.bfloat16
KV_OFFSETS = (
    (2, 2), (1, 2), (2, 1), (3, 2), (2, 3), (1, 1), (3, 3), (1, 3),
    (3, 1), (0, 2), (2, 0), (0, 1), (1, 0), (0, 3), (3, 0),
)
TP_OFFSETS = (
    (4, 0), (4, 1), (3, 0), (5, 0), (3, 1), (5, 1), (2, 0), (6, 0),
    (2, 1), (6, 1), (1, 0), (7, 0), (1, 1), (7, 1), (0, 1),
)
WIDE = 1664


def nt(a, b):
    return lax.dot_general(a, b, (((1,), (1,)), ((), ())), preferred_element_type=F32)


def nn(a, b):
    return jnp.dot(a, b, preferred_element_type=F32)


def kernel(
    tok_hbm, mem_hbm, nrm_hbm, stab_hbm, g1_hbm, wg1_hbm, wu1_hbm, wd1_hbm, g2_hbm,
    wq_hbm, wk_hbm, wv_hbm, wi_hbm, wf_hbm, fb_hbm, wo_hbm, g3_hbm, wg3_hbm, wu3_hbm, wd3_hbm,
    res_ref, memout, newnrm_ref, newstab_ref,
    tok, mem, memb, nrm, stab, g1, wg1, wu1, wd1, g2, wq, wk, wv, wif, fb, wo, g3, wg3, wu3, wd3,
    recv1, blk, send2, recv2, send2b, recv2b, recv3, send4, recv4, send5, recv5, cell, send6, recv6,
    send7, recv7, blk_t, send8, recv8, send8b, recv8b, recv9, wd3t, send10, recv10,
    lsem, ssem, rsem,
):
    kv = lax.axis_index("kv")
    tp = lax.axis_index("tp")
    y, x = kv // 4, kv % 4
    z, core = tp // 2, tp % 2
    kv_peers = [lax.rem(y + dy, 4) * 4 + lax.rem(x + dx, 4) for dy, dx in KV_OFFSETS]
    tp_peers = [lax.rem(z + dz, 8) * 2 + lax.rem(core + dc, 2) for dz, dc in TP_OFFSETS]
    diag = kv == tp
    a_me = jnp.where(core == 1, x, y)
    b_me = jnp.where(core == 1, y, x)
    g_me = a_me * 4 + b_me
    a_peers = [lax.rem(a_me + d, 4) for d in (2, 3, 1)]
    b_peers = [lax.rem(b_me + d, 4) for d in (2, 3, 1)]

    def at(a, b):
        return jnp.where(core == 1, b * 4 + a, a * 4 + b)

    barrier = pltpu.get_barrier_semaphore()
    for t in tp_peers:
        pl.semaphore_signal(barrier, inc=1, device_id=(kv, t), device_id_type=MESH)
    for k in kv_peers:
        pl.semaphore_signal(barrier, inc=1, device_id=(k, tp), device_id_type=MESH)

    pairs = [
        (tok_hbm, tok), (wg1_hbm, wg1), (wu1_hbm, wu1), (g1_hbm, g1), (wd1_hbm, wd1),
        (wq_hbm, wq), (wk_hbm, wk), (wv_hbm, wv), (wi_hbm, wif.at[pl.ds(0, 16)]),
        (wf_hbm, wif.at[pl.ds(16, 16)]), (g2_hbm, g2), (mem_hbm, mem), (nrm_hbm, nrm),
        (stab_hbm, stab), (fb_hbm, fb), (wo_hbm, wo), (g3_hbm, g3), (wg3_hbm, wg3),
        (wu3_hbm, wu3), (wd3_hbm, wd3),
    ]
    loads = [pltpu.make_async_copy(s, d, lsem.at[i]) for i, (s, d) in enumerate(pairs)]
    for c in loads:
        c.start()
    (ld_tok, ld_wg1, ld_wu1, ld_g1, ld_wd1, ld_wq, ld_wk, ld_wv, ld_wi, ld_wf, ld_g2, ld_mem,
     ld_nrm, ld_stab, ld_fb, ld_wo, ld_g3, ld_wg3, ld_wu3, ld_wd3) = loads

    def send(src, dst, sem, k, t):
        pltpu.make_async_remote_copy(
            src_ref=src, dst_ref=dst, send_sem=ssem.at[sem], recv_sem=rsem.at[sem],
            device_id=(k, t), device_id_type=MESH,
        ).start()

    def arrived(buf, sem, count):
        part = buf.at[pl.ds(0, count)]
        pltpu.make_async_copy(part, part, rsem.at[sem]).wait()

    def sent(buf, sem, count):
        part = buf.at[pl.ds(0, count)]
        pltpu.make_async_copy(part, part, ssem.at[sem]).wait()

    def gain_row(g, c):
        return jnp.concatenate([g[pl.ds(2 * c, 1), :], g[pl.ds(2 * c + 1, 1), :]], axis=1)

    spot = lax.broadcasted_iota(jnp.int32, (256, 256), 1)
    seq = lax.broadcasted_iota(jnp.int32, (256, 256), 0)
    spot_row = ((spot % 128) // 8) * 16 + (spot // 128) * 8 + spot % 8
    order = jnp.where(seq == spot_row, 1.0, 0.0).astype(BF16)
    ld_tok.wait()
    ordered = nn(tok[...], order).astype(BF16)
    for h in range(2):
        recv1[h, pl.ds(tp, 1)] = ordered[:, h * 128 : h * 128 + 128][None]
    pl.semaphore_wait(barrier, 30)

    for h in range(2):
        for t in tp_peers:
            send(recv1.at[h, tp], recv1.at[h, tp], h, kv, t)

    def gate_up(h, block, gain, wg, wu, out, into, sem):
        vals = block.astype(F32)
        scaled = (vals * gain).astype(BF16)
        sq = jnp.sum(vals * vals, axis=1, keepdims=True)
        out[h, :, :, pl.ds(1536, 128)] = jnp.broadcast_to(sq, (128, 128)).astype(BF16).reshape(4, 32, 128)
        for n in range(3):
            cols = pl.ds(n * 256, 256)
            out[h, :, :, cols] = nn(scaled, wg[:, cols]).astype(BF16).reshape(4, 32, 256)
            out[h, :, :, pl.ds(768 + n * 256, 256)] = nn(scaled, wu[:, cols]).astype(BF16).reshape(4, 32, 256)
        for a in a_peers:
            send(out.at[h, a], into.at[h, a_me], sem, at(a, b_me), tp)
        into[h, pl.ds(a_me, 1)] = out[h, pl.ds(a_me, 1)]

    def second_sum(h, into, sem, out, next_into, next_sem):
        arrived(into.at[h], sem, 3)
        for n in range(0, WIDE, 128):
            cols = pl.ds(n, 128)
            total = jnp.sum(into[h, :, :, cols].astype(F32), axis=0)
            out[h, :, :, cols] = total.reshape(4, 8, 128).astype(BF16)
        for b in b_peers:
            send(out.at[h, b], next_into.at[h, b_me], next_sem, at(a_me, b), tp)
        next_into[h, pl.ds(b_me, 1)] = out[h, pl.ds(b_me, 1)]

    def hidden(h, into, sem, gathered, next_sem):
        arrived(into.at[h], sem, 3)
        total = jnp.sum(into[h].astype(F32), axis=0)
        scale = lax.rsqrt(total[:, 1536:1537] / 4096 + EPS)
        gate = scale * total[:, :768]
        up = scale * total[:, 768:1536]
        gathered[h, pl.ds(g_me, 1)] = (gate / (1.0 + jnp.exp(-gate)) * up).astype(BF16)[None]
        for k in kv_peers:
            send(gathered.at[h, g_me], gathered.at[h, g_me], next_sem, k, tp)

    def to_group(buf, into, sem):
        for t in tp_peers:
            send(buf, into.at[kv], sem, tp, t)

        @pl.when(jnp.logical_not(diag))
        def _():
            send(buf, into.at[kv], sem, tp, tp)

        @pl.when(diag)
        def _():
            into[pl.ds(kv, 1)] = buf[...][None]

    def from_group(buf, wait, sem):
        @pl.when(diag)
        def _():
            wait(buf, sem, 15)

        @pl.when(jnp.logical_not(diag))
        def _():
            wait(buf, sem, 16)

    gain = None
    for h in range(2):
        arrived(recv1.at[h], h, 15)
        block = recv1[h].reshape(256, 128).T
        blk[h] = block.reshape(16, 8, 256)
        if h == 0:
            ld_wg1.wait()
            ld_wu1.wait()
            ld_g1.wait()
            gain = gain_row(g1, kv)
        gate_up(h, block, gain, wg1, wu1, send2, recv2, 2 + h)
    for h in range(2):
        second_sum(h, recv2, 2 + h, send2b, recv2b, 4 + h)
    for h in range(2):
        hidden(h, recv2b, 4 + h, recv3, 6 + h)

    ld_wd1.wait()
    for h in range(2):
        arrived(recv3.at[h], 6 + h, 15)
        send4[h] = nn(recv3[h].reshape(128, 768), wd1[...]).astype(BF16).reshape(16, 8, 256)
        for t in tp_peers:
            send(send4.at[h, t], recv4.at[h, tp], 8 + h, kv, t)
        recv4[h, pl.ds(tp, 1)] = send4[h, pl.ds(tp, 1)]
    for c in (ld_wq, ld_wk, ld_wv, ld_wi, ld_wf, ld_g2, ld_nrm, ld_stab, ld_fb, ld_mem, ld_wo):
        c.wait()
    memb[...] = mem[...].astype(BF16)

    for h in range(2):
        arrived(recv4.at[h], 8 + h, 15)
        first = jnp.sum(recv4[h].astype(F32), axis=0)
        send5[h] = (blk[h, pl.ds(tp, 1)][0].astype(F32) + 0.5 * first).astype(BF16)
        to_group(send5.at[h], recv5.at[h], 10 + h)
    for h in range(2):
        from_group(recv5.at[h], arrived, 10 + h)

    sq = jnp.zeros((16, 256), F32)
    for c in range(16):
        v = jnp.concatenate([recv5[0, c].astype(F32), recv5[1, c].astype(F32)], axis=0)
        sq = sq + v * v
        cell[:, pl.ds(c * 256, 256)] = (v * gain_row(g2, c)).astype(BF16)
    scale = lax.rsqrt(jnp.sum(sq, axis=1, keepdims=True) / 4096 + EPS)
    query = scale * nn(cell[...], wq[...]) * 128 ** (-0.5)
    key = scale * nn(cell[...], wk[...])
    value = scale * nn(cell[...], wv[...])
    gates = nt(cell[...], wif[...])
    lane32 = lax.broadcasted_iota(jnp.int32, (16, 32), 1)
    input_pre = scale * jnp.sum(jnp.where(lane32 == tp, gates, 0.0), axis=1, keepdims=True)
    pre = scale * jnp.sum(jnp.where(lane32 == tp + 16, gates, 0.0), axis=1, keepdims=True) + fb[...]
    log_forget = jnp.minimum(pre, 0.0) - jnp.log1p(jnp.exp(-jnp.abs(pre)))
    eye = lax.broadcasted_iota(jnp.int32, (16, 16), 0) == lax.broadcasted_iota(jnp.int32, (16, 16), 1)
    old_stab = jnp.sum(jnp.where(eye, jnp.broadcast_to(stab[...], (16, 16)), 0.0), axis=1, keepdims=True)
    carried = log_forget + old_stab
    new_stab = jnp.maximum(carried, input_pre)
    keep = jnp.exp(carried - new_stab)
    admit = jnp.exp(input_pre - new_stab)
    match = jnp.sum(query * key, axis=1, keepdims=True)
    denom = keep * jnp.sum(nrm[...] * query, axis=1, keepdims=True) + admit * match
    qb = query.astype(BF16)
    row256 = lax.broadcasted_iota(jnp.int32, (16, 256), 0)
    recalled = jnp.zeros((16, 256), F32)
    for b in range(16):
        recalled = jnp.where(row256 == b, nt(qb, memb[b]), recalled)
    numer = keep * recalled + (admit * match) * value
    cell_out = (numer / jnp.maximum(jnp.abs(denom), 1.0)).astype(BF16)

    for c in range(16):
        send6[:, c] = nn(cell_out, wo[:, pl.ds(c * 256, 256)]).astype(BF16).reshape(2, 8, 256)
    for h in range(2):
        for t in tp_peers:
            send(send6.at[h, t], recv6.at[h, tp], 12 + h, kv, t)
        recv6[h, pl.ds(tp, 1)] = send6[h, pl.ds(tp, 1)]

    for c in (ld_wg3, ld_wu3, ld_g3, ld_wd3):
        c.wait()
    for h in range(2):
        arrived(recv6.at[h], 12 + h, 15)
        mixed = jnp.sum(recv6[h].astype(F32), axis=0)
        send7[h] = (recv5[h, pl.ds(tp, 1)][0].astype(F32) + mixed).astype(BF16)
        to_group(send7.at[h], recv7.at[h], 14 + h)

    gain = gain_row(g3, kv)
    for h in range(2):
        from_group(recv7.at[h], arrived, 14 + h)
        gate_up(h, recv7[h].reshape(128, 256), gain, wg3, wu3, send8, recv8, 16 + h)
    for h in range(2):
        blk_t[h] = recv7[h].reshape(128, 256).T
    wd3t[...] = wd3[...].T
    newnrm_ref[...] = keep * nrm[...] + admit * key
    newstab_ref[...] = jnp.sum(jnp.where(eye, jnp.broadcast_to(new_stab, (16, 16)), 0.0), axis=0, keepdims=True)
    added = admit * key
    vh = value.astype(BF16)
    vl = (value - vh.astype(F32)).astype(BF16)
    vt = jnp.concatenate([vh.astype(F32), vl.astype(F32), vh.astype(F32)], axis=0).T.astype(BF16)
    row128 = lax.broadcasted_iota(jnp.int32, (16, 128), 0)
    kh = added.astype(BF16).astype(F32)
    kl = added - kh
    for b in range(16):
        khb = jnp.where(row128 == b, kh, 0.0)
        klb = jnp.where(row128 == b, kl, 0.0)
        outer = nn(vt, jnp.concatenate([khb, khb, klb], axis=0).astype(BF16))
        kb = jnp.sum(jnp.where(row128[:, :1] == b, keep, 0.0), axis=0, keepdims=True)
        memout[b] = kb * mem[b] + outer

    for h in range(2):
        second_sum(h, recv8, 16 + h, send8b, recv8b, 18 + h)
    for h in range(2):
        hidden(h, recv8b, 18 + h, recv9, 20 + h)

    for h in range(2):
        arrived(recv9.at[h], 20 + h, 15)
        send10[h] = nt(wd3t[...], recv9[h].reshape(128, 768)).astype(BF16).reshape(16, 16, 128)
        for t in tp_peers:
            send(send10.at[h, t], recv10.at[h, tp], 22 + h, kv, t)
        recv10[h, pl.ds(tp, 1)] = send10[h, pl.ds(tp, 1)]
    halves = []
    rows = pl.ds(pl.multiple_of(tp * 16, 16), 16)
    for h in range(2):
        arrived(recv10.at[h], 22 + h, 15)
        last = jnp.sum(recv10[h].astype(F32), axis=0)
        halves.append((blk_t[h, rows, :].astype(F32) + 0.5 * last).astype(BF16))
    res_ref[...] = nt(jnp.concatenate(halves, axis=1), order).astype(BF16)

    for h in range(2):
        sent(recv1.at[h], h, 15)
        sent(send2.at[h], 2 + h, 3)
        sent(send2b.at[h], 4 + h, 3)
        sent(recv3.at[h], 6 + h, 15)
        sent(send4.at[h], 8 + h, 15)
        from_group(recv5.at[h], sent, 10 + h)
        sent(send6.at[h], 12 + h, 15)
        from_group(recv7.at[h], sent, 14 + h)
        sent(send8.at[h], 16 + h, 3)
        sent(send8b.at[h], 18 + h, 3)
        sent(recv9.at[h], 20 + h, 15)
        sent(send10.at[h], 22 + h, 15)


def finish(res, mem, nrm, stab, res_out, mem_out, nrm_out, stab_out, sem):
    pairs = ((mem, mem_out), (res, res_out), (nrm, nrm_out), (stab, stab_out))
    copies = [pltpu.make_async_copy(s, d, sem.at[i]) for i, (s, d) in enumerate(pairs)]
    for c in copies:
        c.start()
    for c in copies:
        c.wait()


def layer(
    tokens, memory, normalizer, stabilizer, first_gain, first_gate, first_up, first_down, mixer_gain,
    query_weight, key_weight, value_weight, input_weight, forget_weight, forget_bias, output_weight,
    last_gain, last_gate, last_up, last_down,
):
    hbm = pl.BlockSpec(memory_space=pltpu.HBM)
    vmem = pl.BlockSpec(memory_space=pltpu.VMEM)
    b = lambda *s: pltpu.VMEM(s, BF16)
    f = lambda *s: pltpu.VMEM(s, F32)
    wide = lambda *s: b(2, 4, *s, WIDE)
    small = lambda: b(2, 16, 8, 256)
    scratch = [
        b(16, 256), f(16, 256, 128), b(16, 256, 128), f(16, 128), f(1, 16),
        f(32, 128), b(256, 768), b(256, 768), b(768, 256), f(32, 128),
        b(4096, 128), b(4096, 128), b(4096, 256), b(32, 4096), f(1, 1), b(256, 4096),
        f(32, 128), b(256, 768), b(256, 768), b(768, 256),
        b(2, 16, 16, 128), small(), wide(32), wide(32), wide(8), wide(8), b(2, 16, 8, 768),
        small(), small(), b(2, 8, 256), small(), b(16, 4096),
        small(), small(), b(2, 8, 256), small(), b(2, 256, 128),
        wide(32), wide(32), wide(8), wide(8), b(2, 16, 8, 768), b(256, 768),
        b(2, 16, 16, 128), b(2, 16, 16, 128),
        pltpu.SemaphoreType.DMA((20,)), pltpu.SemaphoreType.DMA((24,)), pltpu.SemaphoreType.DMA((24,)),
    ]
    shapes = (((16, 256), BF16), ((16, 256, 128), F32), ((16, 128), F32), ((1, 16), F32))
    parts = pl.pallas_call(
        kernel,
        out_shape=tuple(pltpu.VMEM(*s) for s in shapes),
        in_specs=[hbm] * 20,
        out_specs=(vmem,) * 4,
        scratch_shapes=scratch,
        compiler_params=pltpu.CompilerParams(
            collective_id=0, has_side_effects=True, vmem_limit_bytes=64_900_000
        ),
        name="layer",
    )(*(v for v in (
        tokens.T, memory.reshape(16, 256, 128), normalizer.reshape(16, 128), stabilizer.reshape(1, 16),
        first_gain.reshape(32, 128), first_gate, first_up, first_down, mixer_gain.reshape(32, 128),
        query_weight, key_weight, value_weight, input_weight.T, forget_weight.T,
        forget_bias.reshape(1, 1), output_weight, last_gain.reshape(32, 128), last_gate, last_up, last_down,
    )))
    res, new_mem, new_nrm, new_stab = pl.pallas_call(
        finish,
        out_shape=tuple(jax.ShapeDtypeStruct(*s) for s in shapes),
        in_specs=[vmem] * 4,
        out_specs=(hbm,) * 4,
        scratch_shapes=[pltpu.SemaphoreType.DMA((4,))],
        compiler_params=pltpu.CompilerParams(vmem_limit_bytes=1024 * 1024),
        name="finish",
    )(*(pltpu.with_memory_space_constraint(v, pltpu.VMEM) for v in parts))
    return res.T, new_mem.reshape(16, 1, 256, 128), new_nrm.reshape(16, 1, 128), new_stab.reshape(16, 1)


def solution(mesh):
    in_specs = (
        P(None, ("kv", "tp")), P("kv", "tp", None, None), P("kv", "tp", None), P("kv", "tp"), P(),
        P("kv", "tp"), P("kv", "tp"), P("tp", "kv"), P(), P(None, "tp"), P(None, "tp"), P(None, "tp"),
        P(), P(), P("tp"), P("tp", None), P(), P("kv", "tp"), P("kv", "tp"), P("tp", "kv"),
    )
    out_specs = (P(None, ("kv", "tp")), P("kv", "tp", None, None), P("kv", "tp", None), P("kv", "tp"))
    return jax.shard_map(layer, mesh=mesh, in_specs=in_specs, out_specs=out_specs, check_vma=False)
```
